128 devices in a mesh: sp: 64 (over z, y, x), tp: 2 (over core).
Axes of the slice: x: 4, y: 4, z: 4, core: 2. Of those that a mesh axis runs over, the one named last changes fastest.
Arguments:
- residual: bfloat16 [16384, 2048], P(('sp', 'tp')), may hold values from -6 to 6
- query_one: bfloat16 [16384, 512], P('sp', 'tp'), may hold values from -6.5 to 6.5
- key_one: bfloat16 [16384, 512], P('sp', 'tp'), may hold values from -6.5 to 6.5
- query_two: bfloat16 [16384, 512], P('sp', 'tp'), may hold values from -6.5 to 6.5
- key_two: bfloat16 [16384, 512], P('sp', 'tp'), may hold values from -6.5 to 6.5
- value_rows: bfloat16 [16384, 1024], P('sp', 'tp'), may hold values from -6 to 6
- lambda_head: float32 [8], P('tp'), may hold values from 0.3 to 0.8
- head_gain: float32 [128], replicated, may hold values from 0.1 to 1.9
- out_weight: bfloat16 [1024, 2048], replicated, may hold values from -0.1875 to 0.1875
- norm_gain: float32 [2048], replicated, may hold values from 0.1 to 1.9
- route_ids: int32 [16384, 2], P(('sp', 'tp')), may hold values from 0 to 63, all different within a row; in each aligned block of 128 rows (0 to 127, 128 to 255, ...) at most 6 rows name the same one
- route_weights: float32 [16384, 2], P(('sp', 'tp')), may hold values from 0.25 to 1
- gate_weight: bfloat16 [64, 2048, 512], P('sp', None, 'tp'), may hold values from -0.125 to 0.125
- up_weight: bfloat16 [64, 2048, 512], P('sp', None, 'tp'), may hold values from -0.125 to 0.125
- down_weight: bfloat16 [64, 512, 2048], P('sp', 'tp'), may hold values from -0.25 to 0.25
Outputs:
- mixed: bfloat16 [16384, 2048], P(('sp', 'tp'))
The draws below stay inside these ranges and needn't reach their ends.
Inputs may be any that keep to these rules, and one draw needn't show every extreme that they name: `route_ids`: each row names 2 different experts. Among the rows of one device (aligned blocks of 128 rows) no expert is named more than 6 times, and in every draw some device has an expert named exactly 6 times.
All inputs are finite; a program needn't handle non-finite values.
Results may differ from the reference program's by a relative error of at most 0.014.
Values may be sent and summed in bfloat16 or wider, within the bound.
A program may use at most 128 MiB of HBM per device.

```python
import math
import jax
import jax.numpy as jnp
import numpy as np
from jax import lax

D = 2048
HEADS = 8
HD = 64
VD = 128
FF = 512
TOPK = 2
TOK_DEV = 256
TOKENS = 16384
EXPERTS = 64
CAP = 6
N_SP = 64
N_TP = 2


def draw_queries(key, map_index):
    sample = 1.3 * jax.random.normal(jax.random.fold_in(key, 11 + map_index), (TOKENS, HEADS * HD), jnp.float32)
    sample = jnp.clip(sample, -6.5, 6.5)
    return sample.astype(jnp.bfloat16)


def draw_keys(key, map_index):
    sample = 1.3 * jax.random.normal(jax.random.fold_in(key, 21 + map_index), (TOKENS, HEADS * HD), jnp.float32)
    sample = jnp.clip(sample, -6.5, 6.5)
    return sample.astype(jnp.bfloat16)


def draw_query_one(key, part):
    return draw_queries(key, 0)


def draw_key_one(key, part):
    return draw_keys(key, 0)


def draw_query_two(key, part):
    return draw_queries(key, 1)


def draw_key_two(key, part):
    return draw_keys(key, 1)


def levels(key, dims, shards, least, high):
    gain = 1.0
    for dim, blocks in shards:
        heights = jax.random.uniform(jax.random.fold_in(jax.random.fold_in(key, 6), dim), (blocks,), jnp.float32, least / len(shards), high / len(shards))
        gain = gain * jnp.repeat(jnp.exp(heights), dims[dim] // blocks).reshape((-1,) + (1,) * (len(dims) - 1 - dim))
    return gain


def routed_block(rng, own, number, rows, number_of, top, limit, skew):
    order = jax.random.permutation(rng, number_of)
    packed, ordinary = shares(number_of, rows * top, limit, skew, True), shares(number_of, rows * top, limit, skew, False)
    places = jnp.arange(number_of)

    def named(lengths, turn):
        used = int((lengths > 0).sum())
        fixed = max(1, used // 4)
        shifted = fixed + (places - fixed + turn * (used - fixed)) % max(1, number_of - fixed)
        return jnp.zeros((number_of,), jnp.int32).at[order[jnp.where(places < fixed, places, shifted)]].set(jnp.asarray(lengths, jnp.int32))

    lengths = jnp.where(number % 4 == 0, named(packed, number // 4), named(ordinary, number - number // 4 - 1))
    mixed = jax.random.permutation(jax.random.fold_in(own, 3), number_of)
    giver, taker = mixed[0:number_of // 2 * 2:2], mixed[1:number_of // 2 * 2:2]
    margin = jnp.minimum(lengths[giver] - 1, limit - lengths[taker]) // 2
    margin = jnp.where((giver == order[0]) | (taker == order[0]) | (lengths[taker] == 0), 0, jnp.maximum(margin, 0))
    shifted = jax.random.randint(jax.random.fold_in(own, 4), (number_of // 2,), 0, 1 << 20) % (margin + 1)
    lengths = lengths.at[giver].add(-shifted).at[taker].add(shifted)
    members = jnp.searchsorted(jnp.cumsum(lengths), jnp.arange(rows * top), side="right").astype(jnp.int32)
    grid = members.reshape(top, rows).T
    grid = grid[jax.random.permutation(jax.random.fold_in(own, 1), rows)]
    turn = jax.random.randint(jax.random.fold_in(own, 2), (rows, 1), 0, top)
    return jnp.take_along_axis(grid, (jnp.arange(top)[None, :] + turn) % top, axis=1)


def shares(amount, total, bound, lean, full):
    loads = [(1 << 20) // math.isqrt(standing ** lean) + 1 for standing in range(1, amount + 1)]
    largest = bound if full else min(bound, max(-(-total // amount), total * loads[0] // sum(loads)))
    least = 1 if total - largest >= amount - 1 else 0
    holding, spare = [largest] + [least] * (amount - 1), total - largest - least * (amount - 1)
    while spare > 0:
        candidates = [i for i in range(1, amount) if holding[i] < largest] or [i for i in range(1, amount) if holding[i] < bound]
        whole, budget = sum([loads[i] for i in candidates]), spare
        for i in candidates:
            more = min(bound - holding[i], max(1, budget * loads[i] // whole), spare)
            holding[i] = holding[i] + more
            spare = spare - more
    return np.array(holding)


def normal_values(own_key, dims, width, most, pieces=(), kind=jnp.bfloat16):
    level = levels(own_key, dims, pieces, -0.22, 0.18) if pieces else 1.0
    values = jax.random.normal(own_key, dims, jnp.float32) * width * level
    return jnp.minimum(jnp.maximum(values, -most), most).astype(kind)


def setup_inputs(seed: int = 0) -> dict:
    seeds = jax.random.split(jax.random.key(seed), 16)
    residual = normal_values(seeds[0], (TOKENS, D), 1.0, 6.0, ((0, 128),))
    query_one = draw_query_one(jax.random.fold_in(seeds[15], 71), 0)
    key_one = draw_key_one(jax.random.fold_in(seeds[15], 71), 0)
    query_two = draw_query_two(jax.random.fold_in(seeds[15], 71), 0)
    key_two = draw_key_two(jax.random.fold_in(seeds[15], 71), 0)
    value_rows = normal_values(seeds[5], (TOKENS, HEADS * VD), 1.0, 6.0, ((0, 64), (1, 2)))
    lambda_head = jnp.clip(0.3 + 0.5 * jax.random.uniform(seeds[6], (HEADS,), jnp.float32) ** levels(seeds[6], (HEADS,), ((0, 2),), -0.2, 0.2), 0.3, 0.8)
    head_gain = jnp.clip(1.0 + 0.18 * jax.random.normal(seeds[7], (VD,), jnp.float32), 0.1, 1.9)
    out_weight = normal_values(seeds[8], (HEADS * VD, D), (HEADS * VD) ** -0.5, 0.1875)
    norm_gain = jnp.clip(1.0 + 0.18 * jax.random.normal(seeds[9], (D,), jnp.float32), 0.1, 1.9)
    route_ids_keys = jax.random.split(jax.random.fold_in(seeds[10], 1), TOKENS // (TOK_DEV // N_TP))
    route_ids_turns = jax.random.permutation(jax.random.fold_in(seeds[10], 3), TOKENS // (TOK_DEV // N_TP))
    route_ids = jax.vmap(lambda own, number: routed_block(jax.random.fold_in(seeds[10], 2), own, number, TOK_DEV // N_TP, EXPERTS, TOPK, CAP, 2))(route_ids_keys, route_ids_turns).reshape((TOKENS, TOPK))
    route_weights = jnp.clip(0.25 + 0.75 * jax.random.uniform(seeds[11], (TOKENS, TOPK), jnp.float32) ** levels(seeds[11], (TOKENS, TOPK), ((0, 128),), -0.2, 0.2), 0.25, 1.0)
    gate_weight = normal_values(seeds[12], (EXPERTS, D, FF), D ** -0.5, 0.125, ((0, 64), (2, 2)))
    up_weight = normal_values(seeds[13], (EXPERTS, D, FF), D ** -0.5, 0.125, ((0, 64), (2, 2)))
    down_weight = normal_values(seeds[14], (EXPERTS, FF, D), FF ** -0.5, 0.25, ((0, 64), (1, 2)))
    return dict(residual=residual, query_one=query_one, key_one=key_one, query_two=query_two, key_two=key_two, value_rows=value_rows, lambda_head=lambda_head, head_gain=head_gain, out_weight=out_weight, norm_gain=norm_gain, route_ids=route_ids, route_weights=route_weights, gate_weight=gate_weight, up_weight=up_weight, down_weight=down_weight)


epsilon = 1e-06

def settle(values):
    return lax.optimization_barrier(values.astype(jnp.bfloat16)).astype(jnp.float32)

def head_map(inputs, allowed):
    queries, keys, value_part = inputs
    scores = jnp.dot(queries, keys.T) * HD ** (-0.5)
    scores = jnp.where(allowed, scores, -jnp.inf)
    highest = lax.optimization_barrier(jnp.max(scores, axis=-1, keepdims=True))
    exp_weights = jnp.where(allowed, jnp.exp(scores - highest), 0.0)
    row_total = lax.optimization_barrier(jnp.sum(exp_weights, axis=-1, keepdims=True))
    summed = jnp.dot(settle(exp_weights), value_part)
    return summed / row_total

def one_map(queries, keys, value_part, allowed):
    head_queries = jnp.transpose(queries, (1, 0, 2))
    head_keys = jnp.transpose(keys, (1, 0, 2))
    head_values = jnp.transpose(value_part, (1, 0, 2))
    result = lax.map(lambda inputs: head_map(inputs, allowed), (head_queries, head_keys, head_values))
    return jnp.transpose(result, (1, 0, 2))

def attention(query_one, key_one, query_two, key_two, value_rows, lambda_head, head_gain):
    first_query = query_one.astype(jnp.float32).reshape(TOKENS, HEADS, HD)
    first_key = key_one.astype(jnp.float32).reshape(TOKENS, HEADS, HD)
    second_query = query_two.astype(jnp.float32).reshape(TOKENS, HEADS, HD)
    second_key = key_two.astype(jnp.float32).reshape(TOKENS, HEADS, HD)
    value_part = value_rows.astype(jnp.float32).reshape(TOKENS, HEADS, VD)
    outputs = []
    for segment in range(N_SP):
        begin_row = segment * TOK_DEV
        end_row = begin_row + TOK_DEV
        allowed = (begin_row + jnp.arange(TOK_DEV))[:, None] >= jnp.arange(end_row)[None, :]
        first_out = one_map(first_query[begin_row:end_row], first_key[:end_row], value_part[:end_row], allowed)
        second_out = one_map(second_query[begin_row:end_row], second_key[:end_row], value_part[:end_row], allowed)
        head_out = first_out - lambda_head[None, :, None] * second_out
        normed = head_out * lax.rsqrt(lax.optimization_barrier(jnp.mean(head_out * head_out, axis=-1, keepdims=True)) + epsilon) * head_gain
        outputs.append(normed.reshape(TOK_DEV, HEADS * VD).astype(jnp.bfloat16))
    return jnp.concatenate(outputs, axis=0)

def experts(routed, route_ids, route_weights, gate_weight, up_weight, down_weight):
    flat_ids = route_ids.reshape(-1).astype(jnp.int32)
    flat_weights = route_weights.reshape(-1)
    most_rows = N_SP * N_TP * CAP
    group_width = FF // N_TP

    def expert_step(totals, inputs):
        index, gate_one, up_one, down_one = inputs
        hits = flat_ids == index
        picked = jnp.nonzero(hits, size=most_rows, fill_value=0)[0].astype(jnp.int32)
        valid = jnp.arange(most_rows) < jnp.sum(hits.astype(jnp.int32))
        token_rows = picked // TOPK
        input_rows = routed[token_rows]
        gate = jnp.dot(input_rows, gate_one, preferred_element_type=jnp.float32)
        upper = jnp.dot(input_rows, up_one, preferred_element_type=jnp.float32)
        hidden = (jax.nn.silu(gate) * upper).astype(jnp.bfloat16)
        summed = jnp.zeros((most_rows, D), jnp.float32)
        for group in range(N_TP):
            begin_col = group * group_width
            partial_value = jnp.dot(hidden[:, begin_col:begin_col + group_width], down_one[begin_col:begin_col + group_width], preferred_element_type=jnp.float32)
            summed = summed + settle(partial_value)
        result = settle(summed)
        weight = jnp.where(valid, flat_weights[picked], 0.0)
        totals = totals.at[token_rows].add(weight[:, None] * result)
        return (totals, None)
    steps_in = (jnp.arange(EXPERTS, dtype=jnp.int32), gate_weight, up_weight, down_weight)
    return lax.scan(expert_step, jnp.zeros((TOKENS, D), jnp.float32), steps_in)[0]

def reference(residual, query_one, key_one, query_two, key_two, value_rows, lambda_head, head_gain, out_weight, norm_gain, route_ids, route_weights, gate_weight, up_weight, down_weight):
    attended = attention(query_one, key_one, query_two, key_two, value_rows, lambda_head, head_gain)
    after = (residual.astype(jnp.float32) + jnp.dot(attended, out_weight, preferred_element_type=jnp.float32)).astype(jnp.bfloat16)
    after_float = after.astype(jnp.float32)
    routed = (after_float * lax.rsqrt(lax.optimization_barrier(jnp.mean(after_float * after_float, axis=-1, keepdims=True)) + epsilon) * norm_gain).astype(jnp.bfloat16)
    moe_out = experts(routed, route_ids, route_weights, gate_weight, up_weight, down_weight)
    return (after_float + moe_out).astype(jnp.bfloat16)
```

```python
import functools
import jax
import jax.numpy as jnp
from jax import lax
from jax.experimental import pallas as pl
from jax.experimental.pallas import tpu as pltpu
from jax.sharding import PartitionSpec as P

epsilon = 1e-06
low_value = -1e30
MESH = pl.DeviceIdType.MESH
ROWS = 256
CAP = 6
DIM_BITS = (1, 2, 4)
ORDERS = ((1, 2, 4), (2, 4, 1), (4, 1, 2), (1, 2, 4))


def to_class(p):
    return ((p + 1) // 2) % 2, p // 2


def to_coord(a, g):
    return 2 * g + (a + g) % 2


def sp_of(a, g):
    return to_coord(a[0], g[0]) * 16 + to_coord(a[1], g[1]) * 4 + to_coord(a[2], g[2])


def flipped(a, mask):
    return tuple((a[i] + ((mask >> (2 - i)) & 1)) % 2 for i in range(3))


class Place:
    def __init__(self):
        self.sp = lax.axis_index("sp")
        self.tp = lax.axis_index("tp")
        coords = (self.sp // 16, (self.sp // 4) % 4, self.sp % 4)
        pairs = [to_class(p) for p in coords]
        self.a = tuple(p[0] for p in pairs)
        self.g = tuple(p[1] for p in pairs)
        self.parity = (self.g[0] + self.g[1] + self.g[2]) % 2
        self.head = self.g[0] * 4 + self.g[1] * 2 + self.g[2]

    def source_g(self, j, core):
        gz, gy = j // 2, j % 2
        return (gz, gy, (core + gz + gy) % 2)


def remote(src, dst, send, recv, device):
    return pltpu.make_async_remote_copy(
        src_ref=src, dst_ref=dst, send_sem=send, recv_sem=recv, device_id=device, device_id_type=MESH
    )


def attention_kernel(
    kv_in, q_in, lam_in, gain_in, gate_in, up_in, down_in,
    att_out, gate_out, up_out, down_out,
    kv_all, q_all, lam_all, q_wide, acc, att_send, att_recv,
    s1_send, s1_recv, s2_send, s2_recv, sib_send, sib_recv, att_ssem, att_rsem, w_send, w_recv,
):
    me = Place()
    sibling = (me.sp, 1 - me.tp)
    barrier = pltpu.get_barrier_semaphore()
    count = 0
    for g in range(8):
        chip = sp_of(me.a, (g // 4, (g // 2) % 2, g % 2))
        for core in range(2):
            itself = (chip == me.sp) & (me.tp == core)

            @pl.when(jnp.logical_not(itself))
            def _():
                pl.semaphore_signal(barrier, inc=1, device_id=(chip, core), device_id_type=MESH)

            count += 1
    for bit in DIM_BITS:
        pl.semaphore_signal(
            barrier, inc=1, device_id=(sp_of(flipped(me.a, bit), me.g), me.tp), device_id_type=MESH
        )
        count += 1
    pl.semaphore_wait(barrier, count - 1)

    for hl in range(4):
        chip = sp_of(me.a, (me.tp, hl // 2, hl % 2))
        j = me.g[0] * 2 + me.g[1]
        itself = (chip == me.sp) & (me.parity == me.tp)
        parts = (
            (kv_in.at[hl], kv_all.at[me.sp]),
            (q_in.at[hl], q_all.at[j]),
            (lam_in.at[hl], lam_all.at[j]),
        )

        @pl.when(itself)
        def _():
            for n, (src, dst) in enumerate(parts):
                pltpu.make_async_copy(src, dst, s1_recv.at[n, j]).start()

        @pl.when(jnp.logical_not(itself))
        def _():
            for n, (src, dst) in enumerate(parts):
                remote(src, dst, s1_send.at[n, hl], s1_recv.at[n, j], (chip, me.parity)).start()

    weights = ((gate_in, gate_out), (up_in, up_out), (down_in, down_out))
    w_copies = [remote(a, b, w_send.at[n], w_recv.at[n], sibling) for n, (a, b) in enumerate(weights)]
    for c in w_copies:
        c.start()

    def tile(j, rel, core):
        return kv_all.at[sp_of(flipped(me.a, rel), me.source_g(j, core))]

    def hop(j, rel, bit):
        target = (sp_of(flipped(me.a, bit), me.g), me.tp)
        at = tile(j, rel, me.tp)
        return remote(at, at, s2_send.at[j, rel ^ bit], s2_recv.at[j, rel ^ bit], target)

    def across(j, rel):
        at = tile(j, rel, me.tp)
        return remote(at, at, sib_send.at[j, rel], sib_recv.at[j, rel], sibling)

    for j in range(4):
        pltpu.make_async_copy(q_all.at[j], q_all.at[j], s1_recv.at[1, j]).wait()
        pltpu.make_async_copy(lam_all.at[j], lam_all.at[j], s1_recv.at[2, j]).wait()
        at = tile(j, 0, me.tp)
        pltpu.make_async_copy(at, at, s1_recv.at[0, j]).wait()
        for bit in ORDERS[j]:
            hop(j, 0, bit).start()
        across(j, 0).start()
    for phase in range(3):
        for j in range(4):
            order = ORDERS[j]
            now = order[phase]
            earlier = [0]
            for b in order[:phase]:
                earlier += [r | b for r in earlier]
            for r in earlier:
                rel = r | now
                at = tile(j, rel, me.tp)
                pltpu.make_async_copy(at, at, s2_recv.at[j, rel]).wait()
                for b in order[phase + 1 :]:
                    hop(j, rel, b).start()
                across(j, rel).start()
    for j in range(4):
        for rel in range(8):
            at = tile(j, rel, 1 - me.tp)
            pltpu.make_async_copy(at, at, sib_recv.at[j, rel]).wait()

    for j in range(4):
        full = jnp.concatenate([q_all[j, 0:128, :], q_all[j, 128:256, :]], axis=1)
        row = lax.broadcasted_iota(jnp.int32, (128, 256), 0)
        zero = jnp.zeros_like(full)
        q_wide[j, :, 0:256] = jnp.where(row < 64, full, zero)
        q_wide[j, :, 256:512] = jnp.where(row >= 64, full, zero)

    wide = 2

    def one_tile(j, carry):
        gz, gy = j // 2, j % 2
        own = sp_of(me.a, (gz, gy, (me.tp + gz + gy) % 2))
        acc[...] = jnp.zeros_like(acc)

        def chunk(first, state, masked):
            m, l = state
            keys = jnp.concatenate([kv_all[first + i, 0:256, :] for i in range(wide)], axis=0)
            values = jnp.concatenate(
                [kv_all[first + i, 256 + 128 * b : 384 + 128 * b, :] for i in range(wide) for b in range(2)],
                axis=1,
            )
            s = jnp.dot(keys, q_wide[j], preferred_element_type=jnp.float32)
            if masked:
                key_pos = first * 256 + lax.broadcasted_iota(jnp.int32, s.shape, 0)
                q_pos = own * 256 + lax.broadcasted_iota(jnp.int32, s.shape, 1) % 256
                s = jnp.where(key_pos <= q_pos, s, low_value)
            newest = jnp.maximum(m, jnp.max(s, axis=0, keepdims=True))
            p = jnp.exp(s - newest)
            factor = jnp.exp(m - newest)
            l = l * factor + jnp.sum(p, axis=0, keepdims=True)
            acc[...] = acc[...] * factor + jnp.dot(
                values, p.astype(jnp.bfloat16), preferred_element_type=jnp.float32
            )
            return newest, l

        start = (jnp.full((1, 512), low_value, jnp.float32), jnp.zeros((1, 512), jnp.float32))
        whole = own // wide
        state = lax.fori_loop(0, whole, lambda i, st: chunk(i * wide, st, False), start)
        m, l = chunk(whole * wide, state, True)
        total = acc[...] / l
        for b in range(2):
            first = total[:, 128 * b : 128 * b + 128]
            second = total[:, 256 + 128 * b : 384 + 128 * b]
            out = first - lam_all[0, 0:1, :] * second
            mean = jnp.mean(out * out, axis=0, keepdims=True)
            out = out * lax.rsqrt(mean + epsilon) * gain_in[...]
            att_send[j, b] = out.astype(jnp.bfloat16)
        return carry

    lax.fori_loop(0, 4, one_tile, 0)

    for j in range(4):
        chip = sp_of(me.a, me.source_g(j, me.tp))
        for b in range(2):
            itself = (chip == me.sp) & (me.tp == b)

            @pl.when(itself)
            def _():
                pltpu.make_async_copy(att_send.at[j, b], att_recv.at[me.head], att_rsem.at[me.head]).start()

            @pl.when(jnp.logical_not(itself))
            def _():
                remote(
                    att_send.at[j, b], att_recv.at[me.head], att_ssem.at[j, b], att_rsem.at[me.head], (chip, b)
                ).start()

    for h in range(8):
        pltpu.make_async_copy(att_recv.at[h], att_recv.at[h], att_rsem.at[h]).wait()
        att_out[h] = att_recv[h]

    for j in range(4):
        chip = sp_of(me.a, me.source_g(j, me.tp))
        for b in range(2):

            @pl.when(jnp.logical_not((chip == me.sp) & (me.tp == b)))
            def _():
                pltpu.make_async_copy(att_send.at[j, b], att_send.at[j, b], att_ssem.at[j, b]).wait()

        for rel in range(8):
            if rel:
                at = tile(j, 0, me.tp)
                pltpu.make_async_copy(at, at, s2_send.at[j, rel]).wait()
            at = tile(j, rel, me.tp)
            pltpu.make_async_copy(at, at, sib_send.at[j, rel]).wait()
    for hl in range(4):
        chip = sp_of(me.a, (me.tp, hl // 2, hl % 2))

        @pl.when(jnp.logical_not((chip == me.sp) & (me.parity == me.tp)))
        def _():
            for n, src in enumerate((kv_in, q_in, lam_in)):
                pltpu.make_async_copy(src.at[hl], src.at[hl], s1_send.at[n, hl]).wait()

    for c in w_copies:
        c.wait()


def attention(kv, q, lam, gain, gate, up, down):
    vmem = pl.BlockSpec(memory_space=pltpu.VMEM)
    anywhere = pl.BlockSpec(memory_space=pl.ANY)
    dma = pltpu.SemaphoreType.DMA
    bf16 = jnp.bfloat16
    return pl.pallas_call(
        attention_kernel,
        out_shape=(
            jax.ShapeDtypeStruct((8, 128, 128), bf16),
            jax.ShapeDtypeStruct(gate.shape, bf16),
            jax.ShapeDtypeStruct(up.shape, bf16),
            jax.ShapeDtypeStruct(down.shape, bf16),
        ),
        in_specs=[vmem] * 4 + [anywhere] * 3,
        out_specs=(vmem, anywhere, anywhere, anywhere),
        scratch_shapes=[
            pltpu.VMEM((64, 512, 128), bf16),
            pltpu.VMEM((4, 256, 128), bf16),
            pltpu.VMEM((4, 8, 128), jnp.float32),
            pltpu.VMEM((4, 128, 512), bf16),
            pltpu.VMEM((128, 512), jnp.float32),
            pltpu.VMEM((4, 2, 128, 128), bf16),
            pltpu.VMEM((8, 128, 128), bf16),
            dma((3, 4)), dma((3, 4)), dma((4, 8)), dma((4, 8)), dma((4, 8)), dma((4, 8)),
            dma((4, 2)), dma((8,)), dma((3,)), dma((3,)),
        ],
        compiler_params=pltpu.CompilerParams(
            collective_id=0, has_side_effects=True, vmem_limit_bytes=40 * 1024 * 1024
        ),
    )(kv, q, lam, gain, gate, up, down)


def exchange_kernel(x, y, send, recv, local):
    sp = lax.axis_index("sp")
    tp = lax.axis_index("tp")
    z, yy, xx = sp // 16, (sp // 4) % 4, sp % 4

    def shifted(i, sign):
        dz, dy, dx = i // 16, (i // 4) % 4, i % 4
        return (
            ((z + sign * dz + 4) % 4) * 16 + ((yy + sign * dy + 4) % 4) * 4 + (xx + sign * dx + 4) % 4
        )

    barrier = pltpu.get_barrier_semaphore()

    @pl.loop(1, 64)
    def _(i):
        pl.semaphore_signal(barrier, inc=1, device_id=(shifted(i, 1), tp), device_id_type=MESH)

    mine = pltpu.make_async_copy(x.at[sp], y.at[sp], local)
    mine.start()
    pl.semaphore_wait(barrier, 63)

    def copy(i):
        to = shifted(i, 1)
        return remote(x.at[to], y.at[sp], send.at[i], recv.at[i], (to, tp))

    @pl.loop(1, 64)
    def _(i):
        copy(i).start()

    mine.wait()

    @pl.loop(1, 64)
    def _(i):
        at = y.at[shifted(i, -1)]
        pltpu.make_async_copy(at, at, recv.at[i]).wait()

    @pl.loop(1, 64)
    def _(i):
        copy(i).wait_send()


def exchange(x, number):
    anywhere = pl.BlockSpec(memory_space=pl.ANY)
    return pl.pallas_call(
        exchange_kernel,
        out_shape=jax.ShapeDtypeStruct(x.shape, x.dtype),
        in_specs=[anywhere],
        out_specs=anywhere,
        scratch_shapes=[
            pltpu.SemaphoreType.DMA((64,)), pltpu.SemaphoreType.DMA((64,)), pltpu.SemaphoreType.DMA
        ],
        compiler_params=pltpu.CompilerParams(collective_id=number, has_side_effects=True),
        name=f"exchange{number}",
    )(x)


def expert_hidden(rows, gate_half, up_half):
    gate = jnp.dot(rows, gate_half, preferred_element_type=jnp.float32)
    upper = jnp.dot(rows, up_half, preferred_element_type=jnp.float32)
    return (jax.nn.silu(gate) * upper).astype(jnp.bfloat16)


def on_device(
    residual, query_one, key_one, query_two, key_two, value_rows, lambda_head, head_gain, out_weight,
    norm_gain, route_ids, route_weights, gate_weight, up_weight, down_weight,
):
    rows = query_one.shape[0]
    width = residual.shape[1]
    scale = 64 ** (-0.5)

    def by_head(x, size):
        return x.reshape(rows, 4, size)

    keys = jnp.concatenate([by_head(key_one, 64), by_head(key_two, 64)], axis=2).transpose(1, 0, 2)
    values = value_rows.reshape(2, 128, 4, 128).transpose(2, 0, 3, 1).reshape(4, 256, 128)
    kv = jnp.concatenate([keys, values], axis=1)
    queries = jnp.concatenate([by_head(query_one, 64), by_head(query_two, 64)], axis=2) * jnp.bfloat16(scale)
    q = queries.reshape(2, 128, 4, 128).transpose(2, 0, 3, 1).reshape(4, 256, 128)
    lam = jnp.broadcast_to(lambda_head[:, None, None], (4, 8, 128))
    gain = jnp.broadcast_to(head_gain[:, None], (128, 128))
    attended, gate_other, up_other, down_other = attention(
        kv, q, lam, gain, gate_weight, up_weight, down_weight
    )
    attended = attended.reshape(1024, 128)
    projected = lax.dot_general(
        attended, out_weight, (((0,), (0,)), ((), ())), preferred_element_type=jnp.float32
    )
    after = (residual.astype(jnp.float32) + projected).astype(jnp.bfloat16)
    after_float = after.astype(jnp.float32)
    routed = (
        after_float
        * lax.rsqrt(jnp.mean(after_float * after_float, axis=-1, keepdims=True) + epsilon)
        * norm_gain
    ).astype(jnp.bfloat16)

    local = residual.shape[0]
    expert = jnp.arange(64)[:, None]
    first_hit = route_ids[:, 0][None, :] == expert
    second_hit = route_ids[:, 1][None, :] == expert
    hit = (first_hit | second_hit).astype(jnp.bfloat16)
    before = (jnp.arange(local)[:, None] < jnp.arange(local)[None, :]).astype(jnp.bfloat16)
    rank = jnp.dot(hit, before, preferred_element_type=jnp.float32)
    chosen = (rank[:, None, :] == jnp.arange(CAP, dtype=jnp.float32)[None, :, None]) & (hit[:, None, :] > 0)
    share = (
        jnp.where(first_hit, route_weights[:, 0][None, :], 0.0)
        + jnp.where(second_hit, route_weights[:, 1][None, :], 0.0)
    )
    pick = chosen.astype(jnp.bfloat16).reshape(64 * CAP, local)
    blend = jnp.where(chosen, share[:, None, :], 0.0).reshape(64 * CAP, local)
    blend_high = lax.reduce_precision(blend, 8, 7)
    blend_low = blend - blend_high

    outgoing = jnp.dot(pick, routed, preferred_element_type=jnp.float32).astype(jnp.bfloat16)
    arrived = exchange(outgoing.reshape(64, CAP // 2, 2, width), 1).reshape(64 * CAP, width)
    own = expert_hidden(arrived, gate_weight[0], up_weight[0])
    other = expert_hidden(arrived, gate_other[0], up_other[0])
    made = jnp.dot(own, down_weight[0], preferred_element_type=jnp.float32) + jnp.dot(
        other, down_other[0], preferred_element_type=jnp.float32
    )
    returned = exchange(made.astype(jnp.bfloat16).reshape(64, CAP // 2, 2, width), 2)
    returned = returned.reshape(64 * CAP, width)
    dims = (((0,), (0,)), ((), ()))
    moe_out = lax.dot_general(
        blend_high.astype(jnp.bfloat16), returned, dims, preferred_element_type=jnp.float32
    ) + lax.dot_general(
        blend_low.astype(jnp.bfloat16), returned, dims, preferred_element_type=jnp.float32
    )
    return (after_float + moe_out).astype(jnp.bfloat16)


def solution(mesh):
    placed = (
        P(("sp", "tp"), None),
        P("sp", "tp"),
        P("sp", "tp"),
        P("sp", "tp"),
        P("sp", "tp"),
        P("sp", "tp"),
        P("tp"),
        P(),
        P(),
        P(),
        P(("sp", "tp"), None),
        P(("sp", "tp"), None),
        P("sp", None, "tp"),
        P("sp", None, "tp"),
        P("sp", "tp", None),
    )
    return jax.shard_map(
        on_device, mesh=mesh, in_specs=placed, out_specs=P(("sp", "tp"), None), check_vma=False
    )
```

```python
import jax
import jax.numpy as jnp
from jax import lax
from jax.experimental import pallas as pl
from jax.experimental.pallas import tpu as pltpu
from jax.sharding import PartitionSpec as P

epsilon = 1e-06
low_value = -1e30
MESH = pl.DeviceIdType.MESH
CAP = 6
WIDTH = 2048
SINGLES = (1, 2, 4)
DOUBLES = (3, 5, 6)
ORDERS = ((1, 2, 4), (2, 4, 1), (4, 1, 2), (1, 2, 4))
f32 = jnp.float32
bf16 = jnp.bfloat16


def to_class(p):
    return ((p + 1) // 2) % 2, p // 2


def to_coord(a, g):
    return 2 * g + (a + g) % 2


def sp_of(a, g):
    return to_coord(a[0], g[0]) * 16 + to_coord(a[1], g[1]) * 4 + to_coord(a[2], g[2])


def flipped(a, mask):
    return ((a[0] + mask // 4) % 2, (a[1] + (mask // 2) % 2) % 2, (a[2] + mask % 2) % 2)


class Place:
    def __init__(self):
        self.sp = lax.axis_index("sp")
        self.tp = lax.axis_index("tp")
        coords = (self.sp // 16, (self.sp // 4) % 4, self.sp % 4)
        pairs = [to_class(p) for p in coords]
        self.z = coords[0]
        self.a = tuple(p[0] for p in pairs)
        self.g = tuple(p[1] for p in pairs)
        self.parity = (self.g[0] + self.g[1] + self.g[2]) % 2
        self.head = self.g[0] * 4 + self.g[1] * 2 + self.g[2]

    def source_g(self, j, core):
        gz, gy = j // 2, j % 2
        return (gz, gy, (core + gz + gy) % 2)


def remote(src, dst, send, recv, device):
    return pltpu.make_async_remote_copy(
        src_ref=src, dst_ref=dst, send_sem=send, recv_sem=recv, device_id=device, device_id_type=MESH
    )


def arrival(at, sem):
    pltpu.make_async_copy(at, at, sem).wait()


def iota(shape, dim):
    return lax.broadcasted_iota(jnp.int32, shape, dim)


def layer_kernel(
    q1_in, k1_in, q2_in, k2_in, v_in, lam_in, gain_in, res_in, ng_in, ids_in, rw_in,
    ow_in, gate_in, up_in, down_in,
    out_ref,
    kv_own, q_own, lam_own, kv_all, q_all, lam_all, q_wide, acc, m_ref, l_ref, att_send, att_recv,
    ow, gate, up, down, after, routed, pick, blend, perm, perm_back, out_buf, arr_buf, ret_buf, got_buf,
    s1_send, s1_recv, s2_send, s2_recv, sib_send, sib_recv, att_ssem, att_rsem,
    w_local, w_send, w_recv, d_send, d_recv, r_send, r_recv,
):
    me = Place()
    sibling = (me.sp, 1 - me.tp)
    barrier = pltpu.get_barrier_semaphore()

    @pl.loop(1, 64)
    def _(i):
        pl.semaphore_signal(barrier, inc=1, device_id=((me.sp + i) % 64, me.tp), device_id_type=MESH)

    for g in range(8):
        chip = sp_of(me.a, (g // 4, (g // 2) % 2, g % 2))
        pl.semaphore_signal(barrier, inc=1, device_id=(chip, 1 - me.tp), device_id_type=MESH)

    own_copies = [
        pltpu.make_async_copy(gate_in.at[0], gate.at[0], w_local.at[0]),
        pltpu.make_async_copy(up_in.at[0], up.at[0], w_local.at[1]),
        pltpu.make_async_copy(down_in.at[0], down.at[0], w_local.at[2]),
        pltpu.make_async_copy(ow_in, ow, w_local.at[3]),
    ]
    for c in own_copies:
        c.start()

    lane = iota((256, 128), 1)
    for pair in range(2):
        at = pl.ds(pair * 128, 128)
        k1, k2 = k1_in[:, at].astype(f32), k2_in[:, at].astype(f32)
        q1, q2 = q1_in[:, at].astype(f32) * 0.125, q2_in[:, at].astype(f32) * 0.125
        for odd in range(2):
            hl = pair * 2 + odd
            if odd:
                keys = jnp.where(lane < 64, pltpu.roll(k1, 64, 1), k2)
                queries = jnp.where(lane < 64, pltpu.roll(q1, 64, 1), q2)
            else:
                keys = jnp.where(lane < 64, k1, pltpu.roll(k2, 64, 1))
                queries = jnp.where(lane < 64, q1, pltpu.roll(q2, 64, 1))
            kv_own[hl, 0:256, :] = keys.astype(bf16)
            for b in range(2):
                rows = slice(b * 128, b * 128 + 128)
                value = v_in[rows, hl * 128 : hl * 128 + 128].astype(f32)
                kv_own[hl, 256 + b * 128 : 384 + b * 128, :] = value.T.astype(bf16)
                q_own[hl, rows, :] = queries[rows, :].T.astype(bf16)
            lam_own[hl] = jnp.full((8, 128), lam_in[hl], f32)
    pl.semaphore_wait(barrier, 71)

    j_me = me.g[0] * 2 + me.g[1]
    for hl in range(4):
        chip = sp_of(me.a, (me.tp, hl // 2, hl % 2))
        itself = (chip == me.sp) & (me.parity == me.tp)
        parts = (
            (kv_own.at[hl], kv_all.at[me.sp]),
            (q_own.at[hl], q_all.at[j_me]),
            (lam_own.at[hl], lam_all.at[j_me]),
        )

        @pl.when(itself)
        def _():
            for n, (src, dst) in enumerate(parts):
                pltpu.make_async_copy(src, dst, s1_recv.at[n, j_me]).start()

        @pl.when(jnp.logical_not(itself))
        def _():
            for n, (src, dst) in enumerate(parts):
                remote(src, dst, s1_send.at[n, hl], s1_recv.at[n, j_me], (chip, me.parity)).start()

    ids0, ids1 = ids_in[0:1, :], ids_in[1:2, :]
    rw0, rw1 = rw_in[0:1, :], rw_in[1:2, :]
    upper = jnp.where(iota((128, 128), 0) < iota((128, 128), 1), 1.0, 0.0).astype(bf16)
    small = iota((128, 128), 0)
    for blk in range(4):
        expert = blk * 16 + (small % 32) // 2
        place = (small // 32) * 2 + small % 2
        hit0, hit1 = ids0 == expert, ids1 == expert
        hit = jnp.where(hit0 | hit1, 1.0, 0.0)
        rank = jnp.dot(hit.astype(bf16), upper, preferred_element_type=f32)
        chosen = jnp.where(rank == place.astype(f32), hit, 0.0)
        pick[blk * 128 : blk * 128 + 128, :] = chosen.astype(bf16)
        share = chosen * (jnp.where(hit0, rw0, 0.0) + jnp.where(hit1, rw1, 0.0))
        share = share.T
        high = share.astype(bf16)
        blend[0:128, blk * 128 : blk * 128 + 128] = high
        blend[128:256, blk * 128 : blk * 128 + 128] = (share - high.astype(f32)).astype(bf16)
    ia, ib = iota((256, 256), 0), iota((256, 256), 1)
    packed_a = ((ia // 2) % 16) * 16 + (ia % 2) * 8 + ia // 32
    packed_b = ((ib // 2) % 16) * 16 + (ib % 2) * 8 + ib // 32
    perm[...] = jnp.where(packed_a == ib, 1.0, 0.0).astype(bf16)
    perm_back[...] = jnp.where(packed_b == ia, 1.0, 0.0).astype(bf16)

    w_copies = [
        remote(src.at[0], dst.at[1], w_send.at[n], w_recv.at[n], sibling)
        for n, (src, dst) in enumerate(((gate_in, gate), (up_in, up), (down_in, down)))
    ]

    def tile_at(j, rel, core):
        return sp_of(flipped(me.a, rel), me.source_g(j, core))

    def hop(j, rel, bit):
        target = (sp_of(flipped(me.a, bit), me.g), me.tp)
        at = kv_all.at[tile_at(j, rel, me.tp)]
        return remote(at, at, s2_send.at[j, rel ^ bit], s2_recv.at[j, rel ^ bit], target)

    def across(j, rel):
        at = kv_all.at[tile_at(j, rel, me.tp)]
        return remote(at, at, sib_send.at[j, rel], sib_recv.at[j, rel], sibling)

    for j in range(4):
        arrival(kv_all.at[tile_at(j, 0, me.tp)], s1_recv.at[0, j])
        for bit in ORDERS[j]:
            hop(j, 0, bit).start()
        across(j, 0).start()
    for c in w_copies:
        c.start()

    for j in range(4):
        arrival(q_all.at[j], s1_recv.at[1, j])
        arrival(lam_all.at[j], s1_recv.at[2, j])


    def diagonal(j, carry):
        full = jnp.concatenate([q_all[j, 0:128, :], q_all[j, 128:256, :]], axis=1)
        row = iota((128, 256), 0)
        zero = jnp.zeros_like(full)
        q_wide[j, :, 0:256] = jnp.where(row < 64, full, zero)
        q_wide[j, :, 256:512] = jnp.where(row >= 64, full, zero)
        t = tile_at(j, 0, me.tp)
        s = jnp.dot(kv_all[t, 0:256, :], q_wide[j], preferred_element_type=f32)
        s = jnp.where(iota(s.shape, 0) <= iota(s.shape, 1) % 256, s, low_value)
        m = jnp.max(s, axis=0, keepdims=True)
        p = jnp.exp(s - m)
        m_ref[j] = m
        l_ref[j] = jnp.sum(p, axis=0, keepdims=True)
        values = jnp.concatenate([kv_all[t, 256:384, :], kv_all[t, 384:512, :]], axis=1)
        acc[j] = jnp.dot(values, p.astype(bf16), preferred_element_type=f32)
        return carry

    lax.fori_loop(0, 4, diagonal, 0)

    def scores(t, j):
        return jnp.dot(kv_all[t, 0:256, :], q_wide[j], preferred_element_type=f32)

    def tiles_step(tiles, j):
        m, l = m_ref[j], l_ref[j]
        s = scores(tiles[0], j)
        for i, t in enumerate(tiles):
            following = scores(tiles[i + 1], j) if i + 1 < len(tiles) else None
            newest = jnp.maximum(m, jnp.max(s, axis=0, keepdims=True))
            p = jnp.exp(s - newest)
            factor = jnp.exp(m - newest)
            l = l * factor + jnp.sum(p, axis=0, keepdims=True)
            values = jnp.concatenate([kv_all[t, 256:384, :], kv_all[t, 384:512, :]], axis=1)
            acc[j] = acc[j] * factor + jnp.dot(values, p.astype(bf16), preferred_element_type=f32)
            m, s = newest, following
        m_ref[j] = m
        l_ref[j] = l

    def received(rels, gz):
        for j in (2 * gz, 2 * gz + 1):
            order = ORDERS[j]
            for rel in rels:
                arrival(kv_all.at[tile_at(j, rel, me.tp)], s2_recv.at[j, rel])
                last = max(order.index(b) for b in order if rel & b)
                for b in order[last + 1 :]:
                    hop(j, rel, b).start()
                across(j, rel).start()

    groups = ((2, SINGLES, 0), (5, SINGLES, 1), (8, DOUBLES, 0), (11, DOUBLES, 1), (14, (7,), 0), (15, (7,), 1))

    def unit(n, carry):
        for start, rels, gz_static in groups:

            @pl.when(n == start)
            def _():
                received(rels, gz_static)

        third = (n + 1) % 3
        gz = jnp.where(n < 2, n, jnp.where(n < 14, ((n - 2) // 3) % 2, n - 14))
        single = jnp.where(third == 0, 1, jnp.where(third == 1, 2, 4))
        double = jnp.where(third == 0, 3, jnp.where(third == 1, 5, 6))
        rel = jnp.where(n < 2, 0, jnp.where(n < 8, single, jnp.where(n < 14, double, 7)))
        for half in range(2):
            j = 2 * gz + half
            arrival(kv_all.at[tile_at(j, rel, 1 - me.tp)], sib_recv.at[j, rel])
        a_there = flipped(me.a, rel)
        tiles = [sp_of(a_there, (gz, y, x)) for y in range(2) for x in range(2)]
        far = rel // 4 == 1

        def one_query(j, inner):
            gz_q = j // 2
            same = gz_q == gz
            s_own = tile_at(j, 0, me.tp)
            whole = (gz < gz_q) | (same & far & ((me.a[0] + gz) % 2 == 1))

            @pl.when(whole)
            def _():
                tiles_step(tiles, j)

            @pl.when(same & jnp.logical_not(far))
            def _():
                def one(i, c):
                    t = sp_of(a_there, (gz, i // 2, i % 2))

                    @pl.when(t < s_own)
                    def _():
                        tiles_step([t], j)

                    return c

                lax.fori_loop(0, 4, one, 0)

            return inner

        return lax.fori_loop(0, 4, one_query, carry)

    lax.fori_loop(0, 16, unit, 0)

    def finish(j, carry):
        total = acc[j] / l_ref[j]
        for b in range(2):
            first = total[:, 128 * b : 128 * b + 128]
            second = total[:, 256 + 128 * b : 384 + 128 * b]
            out = first - lam_all[0, 0:1, :] * second
            mean = jnp.mean(out * out, axis=0, keepdims=True)
            out = (out * lax.rsqrt(mean + epsilon)).T * gain_in[...]
            att_send[j, b] = out.astype(bf16)
        chip = tile_at(j, 0, me.tp)
        for b in range(2):
            itself = (chip == me.sp) & (me.tp == b)

            @pl.when(itself)
            def _():
                pltpu.make_async_copy(att_send.at[j, b], att_recv.at[me.head], att_rsem.at[me.head]).start()

            @pl.when(jnp.logical_not(itself))
            def _():
                remote(
                    att_send.at[j, b], att_recv.at[me.head], att_ssem.at[j, b], att_rsem.at[me.head], (chip, b)
                ).start()

        return carry

    lax.fori_loop(0, 4, finish, 0)

    own_copies[3].wait()
    for h in range(8):
        arrival(att_recv.at[h], att_rsem.at[h])
    attended = jnp.concatenate([att_recv[h] for h in range(8)], axis=1)

    def project(n, square):
        at = pl.ds(pl.multiple_of(n * 512, 512), 512)
        value = res_in[:, at].astype(f32) + jnp.dot(attended, ow[:, at], preferred_element_type=f32)
        value = value.astype(bf16)
        after[:, at] = value
        value = value.astype(f32)
        return square + jnp.sum(value * value, axis=1, keepdims=True)

    square = lax.fori_loop(0, 4, project, jnp.zeros((128, 1), f32))
    inverse = lax.rsqrt(square * (1.0 / WIDTH) + epsilon)

    def norm(n, carry):
        at = pl.ds(pl.multiple_of(n * 512, 512), 512)
        routed[:, at] = (after[:, at].astype(f32) * inverse * ng_in[:, at]).astype(bf16)
        return carry

    lax.fori_loop(0, 4, norm, 0)

    def packed(value, into, blk):
        rows = pl.ds(pl.multiple_of(blk * 256, 256), 256)
        for c in range(3):
            stacked = jnp.concatenate(
                [value[c * 32 : c * 32 + 32, k * 256 : k * 256 + 256] for k in range(8)], axis=0
            )
            block = jnp.dot(perm_back[...], stacked, preferred_element_type=f32).astype(bf16)
            into[pl.ds(blk * 16, 16), :, c * 256 : c * 256 + 256] = block.reshape(16, 16, 256)

    def unpacked(source, blk, extra):
        parts = []
        for c in range(3):
            block = source[pl.ds(blk * 16, 16), :, c * 256 : c * 256 + 256].reshape(256, 256)
            parts.append(jnp.dot(perm[...], block, preferred_element_type=f32).astype(bf16))
        columns = []
        for k in range(8):
            pieces = [part[k * 32 : k * 32 + 32, :] for part in parts]
            if extra:
                pieces.append(jnp.zeros((32, 256), bf16))
            columns.append(jnp.concatenate(pieces, axis=0))
        return jnp.concatenate(columns, axis=1)

    def block_of(step):
        shift = jnp.where(step == 2, 3, jnp.where(step == 3, 2, step))
        return (me.z + shift) % 4

    def spread(blk, source, target, ssem, rsem):
        def one(i, carry):
            to = blk * 16 + (me.sp + 15 - i) % 16

            @pl.when(to == me.sp)
            def _():
                pltpu.make_async_copy(source.at[to], target.at[me.sp], rsem.at[me.sp]).start()

            @pl.when(to != me.sp)
            def _():
                remote(source.at[to], target.at[me.sp], ssem.at[to], rsem.at[me.sp], (to, me.tp)).start()

            return carry

        lax.fori_loop(0, 16, one, 0)

    def collect(blk, target, rsem):
        def one(i, carry):
            arrival(target.at[blk * 16 + i], rsem.at[blk * 16 + i])
            return carry

        lax.fori_loop(0, 16, one, 0)

    def dispatch(step, carry):
        blk = block_of(step)
        rows = pl.ds(pl.multiple_of(blk * 128, 128), 128)
        value = jnp.dot(pick[rows, :], routed[...], preferred_element_type=f32).astype(bf16)
        packed(value, out_buf, blk)
        spread(blk, out_buf, arr_buf, d_send, d_recv)
        return carry

    lax.fori_loop(0, 4, dispatch, 0)

    for c in own_copies[:3]:
        c.wait()
    for c in w_copies:
        c.wait()

    def work(step, carry):
        blk = block_of(step)
        collect(blk, arr_buf, d_recv)
        x = unpacked(arr_buf, blk, False)
        hidden = []
        for half in range(2):
            g = jnp.dot(x, gate[half], preferred_element_type=f32)
            u = jnp.dot(x, up[half], preferred_element_type=f32)
            hidden.append((g * jax.nn.sigmoid(g) * u).astype(bf16))
        y = jnp.dot(hidden[0], down[0], preferred_element_type=f32) + jnp.dot(
            hidden[1], down[1], preferred_element_type=f32
        )
        packed(y.astype(bf16), ret_buf, blk)
        spread(blk, ret_buf, got_buf, r_send, r_recv)
        return carry

    lax.fori_loop(0, 4, work, 0)

    made = []
    for blk in range(4):
        collect(blk, got_buf, r_recv)
        made.append(unpacked(got_buf, blk, True))
    for n in range(4):
        at = slice(n * 512, n * 512 + 512)
        column = jnp.concatenate([part[:, at] for part in made], axis=0)
        both = jnp.dot(blend[...], column, preferred_element_type=f32)
        out_ref[:, at] = (after[:, at].astype(f32) + (both[0:128] + both[128:256])).astype(bf16)

    for j in range(4):
        chip = tile_at(j, 0, me.tp)
        for b in range(2):

            @pl.when(jnp.logical_not((chip == me.sp) & (me.tp == b)))
            def _():
                arrival(att_send.at[j, b], att_ssem.at[j, b])

        for rel in range(8):
            if rel:
                arrival(kv_all.at[tile_at(j, 0, me.tp)], s2_send.at[j, rel])
            arrival(kv_all.at[tile_at(j, rel, me.tp)], sib_send.at[j, rel])
    for hl in range(4):
        chip = sp_of(me.a, (me.tp, hl // 2, hl % 2))

        @pl.when(jnp.logical_not((chip == me.sp) & (me.parity == me.tp)))
        def _():
            for n, src in enumerate((kv_own, q_own, lam_own)):
                arrival(src.at[hl], s1_send.at[n, hl])

    @pl.loop(0, 64)
    def _(i):
        @pl.when(i != me.sp)
        def _():
            arrival(out_buf.at[i], d_send.at[i])
            arrival(ret_buf.at[i], r_send.at[i])


def on_device(
    residual, query_one, key_one, query_two, key_two, value_rows, lambda_head, head_gain, out_weight,
    norm_gain, route_ids, route_weights, gate_weight, up_weight, down_weight,
):
    vmem = pl.BlockSpec(memory_space=pltpu.VMEM)
    smem = pl.BlockSpec(memory_space=pltpu.SMEM)
    anywhere = pl.BlockSpec(memory_space=pl.ANY)
    dma = pltpu.SemaphoreType.DMA
    V = pltpu.VMEM
    return pl.pallas_call(
        layer_kernel,
        out_shape=jax.ShapeDtypeStruct(residual.shape, bf16),
        in_specs=[vmem] * 5 + [smem] + [vmem] * 5 + [anywhere] * 4,
        out_specs=vmem,
        scratch_shapes=[
            V((4, 512, 128), bf16), V((4, 256, 128), bf16), V((4, 8, 128), f32),
            V((64, 512, 128), bf16), V((4, 256, 128), bf16), V((4, 8, 128), f32),
            V((4, 128, 512), bf16), V((4, 128, 512), f32), V((4, 1, 512), f32), V((4, 1, 512), f32),
            V((4, 2, 128, 128), bf16), V((8, 128, 128), bf16),
            V((1024, WIDTH), bf16), V((2, WIDTH, 256), bf16), V((2, WIDTH, 256), bf16),
            V((2, 256, WIDTH), bf16), V((128, WIDTH), bf16), V((128, WIDTH), bf16),
            V((512, 128), bf16), V((256, 512), bf16), V((256, 256), bf16), V((256, 256), bf16),
            V((64, 16, 768), bf16), V((64, 16, 768), bf16), V((64, 16, 768), bf16), V((64, 16, 768), bf16),
            dma((3, 4)), dma((3, 4)), dma((4, 8)), dma((4, 8)), dma((4, 8)), dma((4, 8)),
            dma((4, 2)), dma((8,)), dma((4,)), dma((3,)), dma((3,)),
            dma((64,)), dma((64,)), dma((64,)), dma((64,)),
        ],
        compiler_params=pltpu.CompilerParams(
            collective_id=0, has_side_effects=True, vmem_limit_bytes=56 * 1024 * 1024
        ),
        name="layer",
    )(
        query_one, key_one, query_two, key_two, value_rows, lambda_head, head_gain[None, :], residual,
        norm_gain[None, :], route_ids.T, route_weights.T, out_weight, gate_weight, up_weight, down_weight,
    )


def solution(mesh):
    placed = (
        P(("sp", "tp"), None),
        P("sp", "tp"),
        P("sp", "tp"),
        P("sp", "tp"),
        P("sp", "tp"),
        P("sp", "tp"),
        P("tp"),
        P(),
        P(),
        P(),
        P(("sp", "tp"), None),
        P(("sp", "tp"), None),
        P("sp", None, "tp"),
        P("sp", None, "tp"),
        P("sp", "tp", None),
    )
    return jax.shard_map(
        on_device, mesh=mesh, in_specs=placed, out_specs=P(("sp", "tp"), None), check_vma=False
    )
```

```python
import jax
import jax.numpy as jnp
from jax import lax
from jax.experimental import pallas as pl
from jax.experimental.pallas import tpu as pltpu
from jax.sharding import PartitionSpec as P

epsilon = 1e-06
low_value = -1e30
MESH = pl.DeviceIdType.MESH
CAP = 6
WIDTH = 2048
SINGLES = (1, 2, 4)
f32 = jnp.float32
bf16 = jnp.bfloat16


def to_class(p):
    return ((p + 1) // 2) % 2, p // 2


def to_coord(a, g):
    return 2 * g + (a + g) % 2


def sp_of(a, g):
    return to_coord(a[0], g[0]) * 16 + to_coord(a[1], g[1]) * 4 + to_coord(a[2], g[2])


def flipped(a, mask):
    return ((a[0] + mask // 4) % 2, (a[1] + (mask // 2) % 2) % 2, (a[2] + mask % 2) % 2)


class Place:
    def __init__(self):
        self.sp = lax.axis_index("sp")
        self.tp = lax.axis_index("tp")
        coords = (self.sp // 16, (self.sp // 4) % 4, self.sp % 4)
        pairs = [to_class(p) for p in coords]
        self.z = coords[0]
        self.a = tuple(p[0] for p in pairs)
        self.g = tuple(p[1] for p in pairs)
        self.parity = (self.g[0] + self.g[1] + self.g[2]) % 2
        self.head = self.g[0] * 4 + self.g[1] * 2 + self.g[2]

    def source_g(self, j, core):
        gz, gy = j // 2, j % 2
        return (gz, gy, (core + gz + gy) % 2)


def remote(src, dst, send, recv, device):
    return pltpu.make_async_remote_copy(
        src_ref=src, dst_ref=dst, send_sem=send, recv_sem=recv, device_id=device, device_id_type=MESH
    )


def arrival(at, sem):
    pltpu.make_async_copy(at, at, sem).wait()


def iota(shape, dim):
    return lax.broadcasted_iota(jnp.int32, shape, dim)


def layer_kernel(
    q1_in, k1_in, q2_in, k2_in, v_in, lam_in, gain_in, res_in, ng_in, ids_in, rw_in,
    ow_in, gate_in, up_in, down_in,
    out_ref,
    kv_own, q_own, lam_own, kv_all, q_all, lam_all, q_wide, acc, m_ref, l_ref, att_send, att_recv,
    ow, gate, up, down, after, routed, pick, blend, perm, perm_back, out_buf, arr_buf, ret_buf, got_buf,
    s1_send, s1_recv, s2_send, s2_recv, sib_send, sib_recv, att_ssem, att_rsem,
    w_local, w_send, w_recv, d_send, d_recv, r_send, r_recv,
):
    me = Place()
    sibling = (me.sp, 1 - me.tp)
    barrier = pltpu.get_barrier_semaphore()

    @pl.loop(1, 64)
    def _(i):
        pl.semaphore_signal(barrier, inc=1, device_id=((me.sp + i) % 64, me.tp), device_id_type=MESH)

    for g in range(8):
        chip = sp_of(me.a, (g // 4, (g // 2) % 2, g % 2))
        pl.semaphore_signal(barrier, inc=1, device_id=(chip, 1 - me.tp), device_id_type=MESH)

    own_copies = [
        pltpu.make_async_copy(gate_in.at[0], gate.at[0], w_local.at[0]),
        pltpu.make_async_copy(up_in.at[0], up.at[0], w_local.at[1]),
        pltpu.make_async_copy(down_in.at[0], down.at[0], w_local.at[2]),
        pltpu.make_async_copy(ow_in, ow, w_local.at[3]),
    ]
    for c in own_copies:
        c.start()

    lane = iota((256, 128), 1)
    for pair in range(2):
        at = pl.ds(pair * 128, 128)
        k1, k2 = k1_in[:, at].astype(f32), k2_in[:, at].astype(f32)
        q1, q2 = q1_in[:, at].astype(f32) * 0.125, q2_in[:, at].astype(f32) * 0.125
        for odd in range(2):
            hl = pair * 2 + odd
            if odd:
                keys = jnp.where(lane < 64, pltpu.roll(k1, 64, 1), k2)
                queries = jnp.where(lane < 64, pltpu.roll(q1, 64, 1), q2)
            else:
                keys = jnp.where(lane < 64, k1, pltpu.roll(k2, 64, 1))
                queries = jnp.where(lane < 64, q1, pltpu.roll(q2, 64, 1))
            kv_own[hl, 0:256, :] = keys.astype(bf16)
            for b in range(2):
                rows = slice(b * 128, b * 128 + 128)
                value = v_in[rows, hl * 128 : hl * 128 + 128].astype(f32)
                kv_own[hl, 256 + b * 128 : 384 + b * 128, :] = value.T.astype(bf16)
                q_own[hl, rows, :] = queries[rows, :].T.astype(bf16)
            lam_own[hl] = jnp.full((8, 128), lam_in[hl], f32)
    pl.semaphore_wait(barrier, 71)

    j_me = me.g[0] * 2 + me.g[1]

    def first_target(hl):
        chip = sp_of(me.a, (me.tp, hl // 2, hl % 2))
        return chip, (chip == me.sp) & (me.parity == me.tp)

    def first_sends(kinds):
        for i in range(4):
            hl = ((me.g[0] + i // 2) % 2) * 2 + (me.g[1] + i % 2) % 2
            chip, itself = first_target(hl)
            every = (
                (kv_own.at[hl], kv_all.at[me.sp]),
                (q_own.at[hl], q_all.at[j_me]),
                (lam_own.at[hl], lam_all.at[j_me]),
            )

            @pl.when(itself)
            def _():
                for n in kinds:
                    pltpu.make_async_copy(*every[n], s1_recv.at[n, j_me]).start()

            @pl.when(jnp.logical_not(itself))
            def _():
                for n in kinds:
                    remote(*every[n], s1_send.at[n, hl], s1_recv.at[n, j_me], (chip, me.parity)).start()

    first_sends((0,))
    first_sends((1, 2))

    ids0, ids1 = ids_in[0:1, :], ids_in[1:2, :]
    rw0, rw1 = rw_in[0:1, :], rw_in[1:2, :]
    upper = jnp.where(iota((128, 128), 0) < iota((128, 128), 1), 1.0, 0.0).astype(bf16)
    small = iota((128, 128), 0)
    for blk in range(4):
        expert = blk * 16 + (small % 32) // 2
        place = (small // 32) * 2 + small % 2
        hit0, hit1 = ids0 == expert, ids1 == expert
        hit = jnp.where(hit0 | hit1, 1.0, 0.0)
        rank = jnp.dot(hit.astype(bf16), upper, preferred_element_type=f32)
        chosen = jnp.where(rank == place.astype(f32), hit, 0.0)
        pick[blk * 128 : blk * 128 + 128, :] = chosen.astype(bf16)
        share = chosen * (jnp.where(hit0, rw0, 0.0) + jnp.where(hit1, rw1, 0.0))
        share = share.T
        high = share.astype(bf16)
        blend[0:128, blk * 128 : blk * 128 + 128] = high
        blend[128:256, blk * 128 : blk * 128 + 128] = (share - high.astype(f32)).astype(bf16)
    ia, ib = iota((256, 256), 0), iota((256, 256), 1)
    packed_a = ((ia // 2) % 16) * 16 + (ia % 2) * 8 + ia // 32
    packed_b = ((ib // 2) % 16) * 16 + (ib % 2) * 8 + ib // 32
    perm[...] = jnp.where(packed_a == ib, 1.0, 0.0).astype(bf16)
    perm_back[...] = jnp.where(packed_b == ia, 1.0, 0.0).astype(bf16)

    w_copies = [
        remote(src.at[0], dst.at[1], w_send.at[n], w_recv.at[n], sibling)
        for n, (src, dst) in enumerate(((gate_in, gate), (up_in, up), (down_in, down)))
    ]

    def tile_at(j, rel, core):
        return sp_of(flipped(me.a, rel), me.source_g(j, core))

    def hop(j, rel, bit):
        target = (sp_of(flipped(me.a, bit), me.g), me.tp)
        at = kv_all.at[tile_at(j, rel, me.tp)]
        return remote(at, at, s2_send.at[j, rel + bit], s2_recv.at[j, rel + bit], target)

    def source_at(i):
        return ((me.g[1] + i // 2) % 2) * 2 + (me.g[2] + i % 2) % 2

    def bits_of(j):
        first = jnp.where(j == 3, me.tp, j)
        turns = [(first + p) % 3 for p in range(3)]
        return [(k * k + k + 2) // 2 for k in turns]

    def across(j, rel):
        at = kv_all.at[tile_at(j, rel, me.tp)]
        return remote(at, at, sib_send.at[j, rel], sib_recv.at[j, rel], sibling)

    def drain_first():
        for hl in range(4):
            @pl.when(jnp.logical_not(first_target(hl)[1]))
            def _():
                for n, src in enumerate((kv_own, q_own, lam_own)):
                    arrival(src.at[hl], s1_send.at[n, hl])

    def drain_keys():
        for j in range(4):
            for rel in range(8):
                if rel:
                    arrival(kv_all.at[tile_at(j, 0, me.tp)], s2_send.at[j, rel])
                arrival(kv_all.at[tile_at(j, rel, me.tp)], sib_send.at[j, rel])
        drain_first()

    def drain_heads():
        for j in range(4):
            chip = tile_at(j, 0, me.tp)
            for b in range(2):

                @pl.when(jnp.logical_not((chip == me.sp) & (me.tp == b)))
                def _():
                    arrival(att_send.at[j, b], att_ssem.at[j, b])

    def drain_rows(buffer, sem):
        @pl.loop(0, 64)
        def _(i):
            @pl.when(i != me.sp)
            def _():
                arrival(buffer.at[i], sem.at[i])

    for i in range(4):
        j = source_at(i)
        arrival(kv_all.at[tile_at(j, 0, me.tp)], s1_recv.at[0, j])
        for bit in SINGLES:
            hop(j, 0, bit).start()
        across(j, 0).start()
    for c in w_copies:
        c.start()

    def received(level, i):
        j = source_at(i)
        bits = bits_of(j)
        sets = (((0,), (1,), (2,)), ((0, 1), (0, 2), (1, 2)), ((0, 1, 2),))[level]
        for places in sets:
            rel = sum(bits[p] for p in places)
            arrival(kv_all.at[tile_at(j, rel, me.tp)], s2_recv.at[j, rel])
            for p in range(places[-1] + 1, 3):
                hop(j, rel, bits[p]).start()
            across(j, rel).start()

    for j in range(4):
        arrival(q_all.at[j], s1_recv.at[1, j])
        arrival(lam_all.at[j], s1_recv.at[2, j])


    def diagonal(j, carry):
        full = jnp.concatenate([q_all[j, 0:128, :], q_all[j, 128:256, :]], axis=1)
        row = iota((128, 256), 0)
        zero = jnp.zeros_like(full)
        q_wide[j, :, 0:256] = jnp.where(row < 64, full, zero)
        q_wide[j, :, 256:512] = jnp.where(row >= 64, full, zero)
        t = tile_at(j, 0, me.tp)
        s = jnp.dot(kv_all[t, 0:256, :], q_wide[j], preferred_element_type=f32)
        s = jnp.where(iota(s.shape, 0) <= iota(s.shape, 1) % 256, s, low_value)
        m = jnp.max(s, axis=0, keepdims=True)
        p = jnp.exp(s - m)
        m_ref[j] = m
        l_ref[j] = jnp.sum(p, axis=0, keepdims=True)
        values = jnp.concatenate([kv_all[t, 256:384, :], kv_all[t, 384:512, :]], axis=1)
        acc[j] = jnp.dot(values, p.astype(bf16), preferred_element_type=f32)
        return carry

    received(0, 0)
    lax.fori_loop(0, 4, diagonal, 0)

    def tiles_step(tiles, j):
        m, l = m_ref[j], l_ref[j]
        groups_here = [tiles[i : i + 2] for i in range(0, len(tiles), 2)]

        def scores(group):
            keys = jnp.concatenate([kv_all[t, 0:256, :] for t in group], axis=0)
            return jnp.dot(keys, q_wide[j], preferred_element_type=f32)

        s = scores(groups_here[0])
        for i, group in enumerate(groups_here):
            following = scores(groups_here[i + 1]) if i + 1 < len(groups_here) else None
            newest = jnp.maximum(m, jnp.max(s, axis=0, keepdims=True))
            p = jnp.exp(s - newest).astype(bf16)
            factor = jnp.exp(m - newest)
            values = jnp.concatenate(
                [kv_all[t, 256 + 128 * b : 384 + 128 * b, :] for t in group for b in range(2)], axis=1
            )
            values = jnp.concatenate([values, jnp.ones((16, values.shape[1]), bf16)], axis=0)
            product = jnp.dot(values, p, preferred_element_type=f32)
            l = l * factor + product[128:129]
            acc[j] = acc[j] * factor + product[0:128]
            m, s = newest, following
        m_ref[j] = m
        l_ref[j] = l

    tasks = ((0, 0, 1), (1, 0, 2), (2, 0, 3), (4, 1, 0), (5, 1, 1), (6, 1, 2), (7, 1, 3),
             (9, 2, 0), (10, 2, 1), (11, 2, 2), (12, 2, 3))

    def unit(n, carry):
        for start, level, i in tasks:

            @pl.when(n == start)
            def _():
                received(level, i)

        third = (n + 1) % 3
        turn = jnp.where(n < 2, n, jnp.where(n < 14, ((n - 2) // 3) % 2, n - 14))
        gz = (turn + me.g[1]) % 2
        single = jnp.where(third == 0, 1, jnp.where(third == 1, 2, 4))
        double = jnp.where(third == 0, 3, jnp.where(third == 1, 5, 6))
        rel = jnp.where(n < 2, 0, jnp.where(n < 8, single, jnp.where(n < 14, double, 7)))
        for half in range(2):
            j = 2 * gz + half
            arrival(kv_all.at[tile_at(j, rel, 1 - me.tp)], sib_recv.at[j, rel])
        a_there = flipped(me.a, rel)
        tiles = [sp_of(a_there, (gz, y, x)) for y in range(2) for x in range(2)]
        far = rel // 4 == 1

        def one_query(j, inner):
            gz_q = j // 2
            same = gz_q == gz
            s_own = tile_at(j, 0, me.tp)
            whole = (gz < gz_q) | (same & far & ((me.a[0] + gz) % 2 == 1))

            near = same & jnp.logical_not(far)
            upper_q = j % 2 == 1
            side = (rel // 2) % 2 == 1
            fits = (me.a[1] + j % 2) % 2 == 1

            @pl.when(whole | (near & side & upper_q & fits))
            def _():
                tiles_step(tiles, j)

            @pl.when(near & ((side & (upper_q != fits)) | (jnp.logical_not(side) & upper_q)))
            def _():
                tiles_step(tiles[0:2], j)

            @pl.when(near & jnp.logical_not(side))
            def _():
                def one(i, c):
                    t = sp_of(a_there, (gz, j % 2, i))

                    @pl.when(t < s_own)
                    def _():
                        tiles_step([t], j)

                    return c

                lax.fori_loop(0, 2, one, 0)

            return inner

        return lax.fori_loop(0, 4, one_query, carry)

    lax.fori_loop(0, 16, unit, 0)

    def finish(j, carry):
        total = acc[j] / l_ref[j]
        for b in range(2):
            first = total[:, 128 * b : 128 * b + 128]
            second = total[:, 256 + 128 * b : 384 + 128 * b]
            out = first - lam_all[0, 0:1, :] * second
            mean = jnp.mean(out * out, axis=0, keepdims=True)
            out = (out * lax.rsqrt(mean + epsilon)).T * gain_in[...]
            att_send[j, b] = out.astype(bf16)
        chip = tile_at(j, 0, me.tp)
        for b in range(2):
            itself = (chip == me.sp) & (me.tp == b)

            @pl.when(itself)
            def _():
                pltpu.make_async_copy(att_send.at[j, b], att_recv.at[me.head], att_rsem.at[me.head]).start()

            @pl.when(jnp.logical_not(itself))
            def _():
                remote(
                    att_send.at[j, b], att_recv.at[me.head], att_ssem.at[j, b], att_rsem.at[me.head], (chip, b)
                ).start()

        return carry

    lax.fori_loop(0, 4, finish, 0)

    own_copies[3].wait()
    for h in range(8):
        arrival(att_recv.at[h], att_rsem.at[h])
    attended = jnp.concatenate([att_recv[h] for h in range(8)], axis=1)

    def project(n, square):
        at = pl.ds(pl.multiple_of(n * 512, 512), 512)
        value = res_in[:, at].astype(f32) + jnp.dot(attended, ow[:, at], preferred_element_type=f32)
        value = value.astype(bf16)
        after[:, at] = value
        value = value.astype(f32)
        return square + jnp.sum(value * value, axis=1, keepdims=True)

    square = lax.fori_loop(0, 4, project, jnp.zeros((128, 1), f32))
    inverse = lax.rsqrt(square * (1.0 / WIDTH) + epsilon)

    def norm(n, carry):
        at = pl.ds(pl.multiple_of(n * 512, 512), 512)
        routed[:, at] = (after[:, at].astype(f32) * inverse * ng_in[:, at]).astype(bf16)
        return carry

    lax.fori_loop(0, 4, norm, 0)

    def packed(value, into, blk):
        rows = pl.ds(pl.multiple_of(blk * 256, 256), 256)
        for c in range(3):
            stacked = jnp.concatenate(
                [value[c * 32 : c * 32 + 32, k * 256 : k * 256 + 256] for k in range(8)], axis=0
            )
            block = jnp.dot(perm_back[...], stacked, preferred_element_type=f32).astype(bf16)
            into[pl.ds(blk * 16, 16), :, c * 256 : c * 256 + 256] = block.reshape(16, 16, 256)

    def unpacked(source, blk, extra):
        parts = []
        for c in range(3):
            block = source[pl.ds(blk * 16, 16), :, c * 256 : c * 256 + 256].reshape(256, 256)
            parts.append(jnp.dot(perm[...], block, preferred_element_type=f32).astype(bf16))
        columns = []
        for k in range(8):
            pieces = [part[k * 32 : k * 32 + 32, :] for part in parts]
            if extra:
                pieces.append(jnp.zeros((32, 256), bf16))
            columns.append(jnp.concatenate(pieces, axis=0))
        return jnp.concatenate(columns, axis=1)

    def block_of(step):
        shift = jnp.where(step == 2, 3, jnp.where(step == 3, 2, step))
        return (me.z + shift) % 4

    def spread(blk, source, target, ssem, rsem):
        def one(i, carry):
            to = blk * 16 + (me.sp + 15 - i) % 16

            @pl.when(to == me.sp)
            def _():
                pltpu.make_async_copy(source.at[to], target.at[me.sp], rsem.at[me.sp]).start()

            @pl.when(to != me.sp)
            def _():
                remote(source.at[to], target.at[me.sp], ssem.at[to], rsem.at[me.sp], (to, me.tp)).start()

            return carry

        lax.fori_loop(0, 16, one, 0)

    def collect(blk, target, rsem):
        def one(i, carry):
            arrival(target.at[blk * 16 + i], rsem.at[blk * 16 + i])
            return carry

        lax.fori_loop(0, 16, one, 0)

    def dispatch(step, carry):
        blk = block_of(step)
        rows = pl.ds(pl.multiple_of(blk * 128, 128), 128)
        value = jnp.dot(pick[rows, :], routed[...], preferred_element_type=f32).astype(bf16)
        packed(value, out_buf, blk)
        spread(blk, out_buf, arr_buf, d_send, d_recv)
        return carry

    lax.fori_loop(0, 4, dispatch, 0)

    for c in own_copies[:3]:
        c.wait()
    for c in w_copies:
        c.wait()

    def work(step, carry):
        blk = block_of(step)
        collect(blk, arr_buf, d_recv)
        x = unpacked(arr_buf, blk, False)
        hidden = []
        for half in range(2):
            g = jnp.dot(x, gate[half], preferred_element_type=f32)
            u = jnp.dot(x, up[half], preferred_element_type=f32)
            hidden.append((g * jax.nn.sigmoid(g) * u).astype(bf16))
        y = jnp.dot(hidden[0], down[0], preferred_element_type=f32) + jnp.dot(
            hidden[1], down[1], preferred_element_type=f32
        )
        packed(y.astype(bf16), ret_buf, blk)
        spread(blk, ret_buf, got_buf, r_send, r_recv)
        return carry

    lax.fori_loop(0, 4, work, 0)

    made = []
    for blk in range(4):
        collect(blk, got_buf, r_recv)
        made.append(unpacked(got_buf, blk, True))
    for n in range(4):
        at = slice(n * 512, n * 512 + 512)
        column = jnp.concatenate([part[:, at] for part in made], axis=0)
        both = jnp.dot(blend[...], column, preferred_element_type=f32)
        out_ref[:, at] = (after[:, at].astype(f32) + (both[0:128] + both[128:256])).astype(bf16)

    drain_heads()
    drain_keys()
    drain_rows(out_buf, d_send)
    drain_rows(ret_buf, r_send)


def on_device(
    residual, query_one, key_one, query_two, key_two, value_rows, lambda_head, head_gain, out_weight,
    norm_gain, route_ids, route_weights, gate_weight, up_weight, down_weight,
):
    vmem = pl.BlockSpec(memory_space=pltpu.VMEM)
    smem = pl.BlockSpec(memory_space=pltpu.SMEM)
    anywhere = pl.BlockSpec(memory_space=pl.ANY)
    dma = pltpu.SemaphoreType.DMA
    V = pltpu.VMEM
    return pl.pallas_call(
        layer_kernel,
        out_shape=jax.ShapeDtypeStruct(residual.shape, bf16),
        in_specs=[vmem] * 5 + [smem] + [vmem] * 5 + [anywhere] * 4,
        out_specs=vmem,
        scratch_shapes=[
            V((4, 512, 128), bf16), V((4, 256, 128), bf16), V((4, 8, 128), f32),
            V((64, 512, 128), bf16), V((4, 256, 128), bf16), V((4, 8, 128), f32),
            V((4, 128, 512), bf16), V((4, 128, 512), f32), V((4, 1, 512), f32), V((4, 1, 512), f32),
            V((4, 2, 128, 128), bf16), V((8, 128, 128), bf16),
            V((1024, WIDTH), bf16), V((2, WIDTH, 256), bf16), V((2, WIDTH, 256), bf16),
            V((2, 256, WIDTH), bf16), V((128, WIDTH), bf16), V((128, WIDTH), bf16),
            V((512, 128), bf16), V((256, 512), bf16), V((256, 256), bf16), V((256, 256), bf16),
            V((64, 16, 768), bf16), V((64, 16, 768), bf16), V((64, 16, 768), bf16), V((64, 16, 768), bf16),
            dma((3, 4)), dma((3, 4)), dma((4, 8)), dma((4, 8)), dma((4, 8)), dma((4, 8)),
            dma((4, 2)), dma((8,)), dma((4,)), dma((3,)), dma((3,)),
            dma((64,)), dma((64,)), dma((64,)), dma((64,)),
        ],
        compiler_params=pltpu.CompilerParams(
            collective_id=0, has_side_effects=True, vmem_limit_bytes=56 * 1024 * 1024
        ),
        name="layer",
    )(
        query_one, key_one, query_two, key_two, value_rows, lambda_head, head_gain[None, :], residual,
        norm_gain[None, :], route_ids.T, route_weights.T, out_weight, gate_weight, up_weight, down_weight,
    )


def solution(mesh):
    placed = (
        P(("sp", "tp"), None),
        P("sp", "tp"),
        P("sp", "tp"),
        P("sp", "tp"),
        P("sp", "tp"),
        P("sp", "tp"),
        P("tp"),
        P(),
        P(),
        P(),
        P(("sp", "tp"), None),
        P(("sp", "tp"), None),
        P("sp", None, "tp"),
        P("sp", None, "tp"),
        P("sp", "tp", None),
    )
    return jax.shard_map(
        on_device, mesh=mesh, in_specs=placed, out_specs=P(("sp", "tp"), None), check_vma=False
    )
```

```python
import jax
import jax.numpy as jnp
from jax import lax
from jax.experimental import pallas as pl
from jax.experimental.pallas import tpu as pltpu
from jax.sharding import PartitionSpec as P

epsilon = 1e-06
low_value = -1e30
MESH = pl.DeviceIdType.MESH
CAP = 6
WIDTH = 2048
SINGLES = (1, 2, 4)
f32 = jnp.float32
bf16 = jnp.bfloat16


def to_class(p):
    return ((p + 1) // 2) % 2, p // 2


def to_coord(a, g):
    return 2 * g + (a + g) % 2


def sp_of(a, g):
    return to_coord(a[0], g[0]) * 16 + to_coord(a[1], g[1]) * 4 + to_coord(a[2], g[2])


def flipped(a, mask):
    return ((a[0] + mask // 4) % 2, (a[1] + (mask // 2) % 2) % 2, (a[2] + mask % 2) % 2)


class Place:
    def __init__(self):
        self.sp = lax.axis_index("sp")
        self.tp = lax.axis_index("tp")
        coords = (self.sp // 16, (self.sp // 4) % 4, self.sp % 4)
        pairs = [to_class(p) for p in coords]
        self.z = coords[0]
        self.a = tuple(p[0] for p in pairs)
        self.g = tuple(p[1] for p in pairs)
        self.parity = (self.g[0] + self.g[1] + self.g[2]) % 2
        self.head = self.g[0] * 4 + self.g[1] * 2 + self.g[2]

    def source_g(self, j, core):
        gz, gy = j // 2, j % 2
        return (gz, gy, (core + gz + gy) % 2)


def remote(src, dst, send, recv, device):
    return pltpu.make_async_remote_copy(
        src_ref=src, dst_ref=dst, send_sem=send, recv_sem=recv, device_id=device, device_id_type=MESH
    )


def arrival(at, sem):
    pltpu.make_async_copy(at, at, sem).wait()


def iota(shape, dim):
    return lax.broadcasted_iota(jnp.int32, shape, dim)


def layer_kernel(
    q1_in, k1_in, q2_in, k2_in, v_in, lam_in, gain_in, res_in, ng_in, ids_in, rw_in,
    ow_in, gate_in, up_in, down_in,
    out_ref,
    kv_own, q_own, lam_own, kv_all, q_all, lam_all, q_wide, acc, m_ref, l_ref, att_send, att_recv,
    ow, gate, up, down, after, routed, pick, blend, perm, perm_back, out_buf, arr_buf, ret_buf, got_buf,
    s1_send, s1_recv, s2_send, s2_recv, sib_send, sib_recv, att_ssem, att_rsem,
    w_local, w_send, w_recv, d_send, d_recv, r_send, r_recv,
):
    me = Place()
    sibling = (me.sp, 1 - me.tp)
    barrier = pltpu.get_barrier_semaphore()

    @pl.loop(1, 64)
    def _(i):
        pl.semaphore_signal(barrier, inc=1, device_id=((me.sp + i) % 64, me.tp), device_id_type=MESH)

    for g in range(8):
        chip = sp_of(me.a, (g // 4, (g // 2) % 2, g % 2))
        pl.semaphore_signal(barrier, inc=1, device_id=(chip, 1 - me.tp), device_id_type=MESH)

    own_copies = [
        pltpu.make_async_copy(gate_in.at[0], gate.at[0], w_local.at[0]),
        pltpu.make_async_copy(up_in.at[0], up.at[0], w_local.at[1]),
        pltpu.make_async_copy(down_in.at[0], down.at[0], w_local.at[2]),
        pltpu.make_async_copy(ow_in, ow, w_local.at[3]),
    ]
    for c in own_copies:
        c.start()

    lane = iota((256, 128), 1)
    for pair in range(2):
        at = pl.ds(pair * 128, 128)
        k1, k2 = k1_in[:, at].astype(f32), k2_in[:, at].astype(f32)
        q1, q2 = q1_in[:, at].astype(f32) * 0.125, q2_in[:, at].astype(f32) * 0.125
        for odd in range(2):
            hl = pair * 2 + odd
            if odd:
                keys = jnp.where(lane < 64, pltpu.roll(k1, 64, 1), k2)
                queries = jnp.where(lane < 64, pltpu.roll(q1, 64, 1), q2)
            else:
                keys = jnp.where(lane < 64, k1, pltpu.roll(k2, 64, 1))
                queries = jnp.where(lane < 64, q1, pltpu.roll(q2, 64, 1))
            kv_own[hl, 0:256, :] = keys.astype(bf16)
            for b in range(2):
                rows = slice(b * 128, b * 128 + 128)
                value = v_in[rows, hl * 128 : hl * 128 + 128].astype(f32)
                kv_own[hl, 256 + b * 128 : 384 + b * 128, :] = value.T.astype(bf16)
                q_own[hl, rows, :] = queries[rows, :].T.astype(bf16)
            lam_own[hl] = jnp.full((8, 128), lam_in[hl], f32)
    pl.semaphore_wait(barrier, 71)

    j_me = me.g[0] * 2 + me.g[1]

    def first_target(hl):
        chip = sp_of(me.a, (me.tp, hl // 2, hl % 2))
        return chip, (chip == me.sp) & (me.parity == me.tp)

    def first_sends(kinds):
        for i in range(4):
            hl = ((me.g[0] + i // 2) % 2) * 2 + (me.g[1] + i % 2) % 2
            chip, itself = first_target(hl)
            every = (
                (kv_own.at[hl], kv_all.at[me.sp]),
                (q_own.at[hl], q_all.at[j_me]),
                (lam_own.at[hl], lam_all.at[j_me]),
            )

            @pl.when(itself)
            def _():
                for n in kinds:
                    pltpu.make_async_copy(*every[n], s1_recv.at[n, j_me]).start()

            @pl.when(jnp.logical_not(itself))
            def _():
                for n in kinds:
                    remote(*every[n], s1_send.at[n, hl], s1_recv.at[n, j_me], (chip, me.parity)).start()

    first_sends((0,))
    first_sends((1, 2))

    ids0, ids1 = ids_in[0:1, :], ids_in[1:2, :]
    rw0, rw1 = rw_in[0:1, :], rw_in[1:2, :]
    upper = jnp.where(iota((128, 128), 0) < iota((128, 128), 1), 1.0, 0.0).astype(bf16)
    small = iota((128, 128), 0)
    for blk in range(4):
        expert = blk * 16 + (small % 32) // 2
        place = (small // 32) * 2 + small % 2
        hit0, hit1 = ids0 == expert, ids1 == expert
        hit = jnp.where(hit0 | hit1, 1.0, 0.0)
        rank = jnp.dot(hit.astype(bf16), upper, preferred_element_type=f32)
        chosen = jnp.where(rank == place.astype(f32), hit, 0.0)
        pick[blk * 128 : blk * 128 + 128, :] = chosen.astype(bf16)
        share = chosen * (jnp.where(hit0, rw0, 0.0) + jnp.where(hit1, rw1, 0.0))
        share = share.T
        high = share.astype(bf16)
        blend[0:128, blk * 128 : blk * 128 + 128] = high
        blend[128:256, blk * 128 : blk * 128 + 128] = (share - high.astype(f32)).astype(bf16)
    ia, ib = iota((256, 256), 0), iota((256, 256), 1)
    packed_a = ((ia // 2) % 16) * 16 + (ia % 2) * 8 + ia // 32
    packed_b = ((ib // 2) % 16) * 16 + (ib % 2) * 8 + ib // 32
    perm[...] = jnp.where(packed_a == ib, 1.0, 0.0).astype(bf16)
    perm_back[...] = jnp.where(packed_b == ia, 1.0, 0.0).astype(bf16)

    w_copies = [
        remote(src.at[0], dst.at[1], w_send.at[n], w_recv.at[n], sibling)
        for n, (src, dst) in enumerate(((gate_in, gate), (up_in, up), (down_in, down)))
    ]

    def tile_at(j, rel, core):
        return sp_of(flipped(me.a, rel), me.source_g(j, core))

    def hop(j, rel, bit):
        target = (sp_of(flipped(me.a, bit), me.g), me.tp)
        at = kv_all.at[tile_at(j, rel, me.tp)]
        return remote(at, at, s2_send.at[j, rel + bit], s2_recv.at[j, rel + bit], target)

    def source_at(i):
        return ((me.g[1] + i // 2) % 2) * 2 + (me.g[2] + i % 2) % 2

    def bits_of(j):
        first = jnp.where(j == 3, me.tp, j)
        turns = [(first + p) % 3 for p in range(3)]
        return [(k * k + k + 2) // 2 for k in turns]

    def across(j, rel):
        at = kv_all.at[tile_at(j, rel, me.tp)]
        return remote(at, at, sib_send.at[j, rel], sib_recv.at[j, rel], sibling)

    def drain_first():
        for hl in range(4):
            @pl.when(jnp.logical_not(first_target(hl)[1]))
            def _():
                for n, src in enumerate((kv_own, q_own, lam_own)):
                    arrival(src.at[hl], s1_send.at[n, hl])

    def drain_keys():
        for j in range(4):
            for rel in range(8):
                if rel:
                    arrival(kv_all.at[tile_at(j, 0, me.tp)], s2_send.at[j, rel])
                arrival(kv_all.at[tile_at(j, rel, me.tp)], sib_send.at[j, rel])
        drain_first()

    def drain_heads():
        for j in range(4):
            chip = tile_at(j, 0, me.tp)
            for b in range(2):

                @pl.when(jnp.logical_not((chip == me.sp) & (me.tp == b)))
                def _():
                    arrival(att_send.at[j, b], att_ssem.at[j, b])

    def drain_rows(buffer, sem):
        @pl.loop(0, 64)
        def _(i):
            @pl.when(i != me.sp)
            def _():
                arrival(buffer.at[i], sem.at[i])

    for i in range(4):
        j = source_at(i)
        arrival(kv_all.at[tile_at(j, 0, me.tp)], s1_recv.at[0, j])
        for bit in SINGLES:
            hop(j, 0, bit).start()
        across(j, 0).start()
    for c in w_copies:
        c.start()

    def received(level, i):
        j = source_at(i)
        bits = bits_of(j)
        sets = (((0,), (1,), (2,)), ((0, 1), (0, 2), (1, 2)), ((0, 1, 2),))[level]
        for places in sets:
            rel = sum(bits[p] for p in places)
            arrival(kv_all.at[tile_at(j, rel, me.tp)], s2_recv.at[j, rel])
            for p in range(places[-1] + 1, 3):
                hop(j, rel, bits[p]).start()
            across(j, rel).start()

    for j in range(4):
        arrival(q_all.at[j], s1_recv.at[1, j])
        arrival(lam_all.at[j], s1_recv.at[2, j])


    def diagonal(j, carry):
        full = jnp.concatenate([q_all[j, 0:128, :], q_all[j, 128:256, :]], axis=1)
        row = iota((128, 256), 0)
        zero = jnp.zeros_like(full)
        q_wide[j, :, 0:256] = jnp.where(row < 64, full, zero)
        q_wide[j, :, 256:512] = jnp.where(row >= 64, full, zero)
        t = tile_at(j, 0, me.tp)
        s = jnp.dot(kv_all[t, 0:256, :], q_wide[j], preferred_element_type=f32)
        s = jnp.where(iota(s.shape, 0) <= iota(s.shape, 1) % 256, s, low_value)
        m = jnp.max(s, axis=0, keepdims=True)
        p = jnp.exp(s - m)
        m_ref[j] = m
        l_ref[j] = jnp.sum(p, axis=0, keepdims=True)
        values = jnp.concatenate([kv_all[t, 256:384, :], kv_all[t, 384:512, :]], axis=1)
        acc[j] = jnp.dot(values, p.astype(bf16), preferred_element_type=f32)
        return carry

    received(0, 0)
    lax.fori_loop(0, 4, diagonal, 0)

    def tiles_step(tiles, j):
        m, l = m_ref[j], l_ref[j]
        groups_here = [tiles[i : i + 2] for i in range(0, len(tiles), 2)]

        def scores(group):
            keys = jnp.concatenate([kv_all[t, 0:256, :] for t in group], axis=0)
            return jnp.dot(keys, q_wide[j], preferred_element_type=f32)

        s = scores(groups_here[0])
        for i, group in enumerate(groups_here):
            following = scores(groups_here[i + 1]) if i + 1 < len(groups_here) else None
            newest = jnp.maximum(m, jnp.max(s, axis=0, keepdims=True))
            p = jnp.exp(s - newest).astype(bf16)
            factor = jnp.exp(m - newest)
            values = jnp.concatenate(
                [kv_all[t, 256 + 128 * b : 384 + 128 * b, :] for t in group for b in range(2)], axis=1
            )
            values = jnp.concatenate([values, jnp.ones((16, values.shape[1]), bf16)], axis=0)
            product = jnp.dot(values, p, preferred_element_type=f32)
            l = l * factor + product[128:129]
            acc[j] = acc[j] * factor + product[0:128]
            m, s = newest, following
        m_ref[j] = m
        l_ref[j] = l

    tasks = ((0, 0, 1), (1, 0, 2), (2, 0, 3), (4, 1, 0), (5, 1, 1), (6, 1, 2), (7, 1, 3),
             (9, 2, 0), (10, 2, 1), (11, 2, 2), (12, 2, 3))

    def pair_step(tiles, first):
        second = first + 1
        m = jnp.concatenate([m_ref[first], m_ref[second]], axis=1)
        l = jnp.concatenate([l_ref[first], l_ref[second]], axis=1)
        queries = jnp.concatenate([q_wide[first], q_wide[second]], axis=1)
        groups_here = [tiles[i : i + 2] for i in range(0, len(tiles), 2)]

        def scores(group):
            keys = jnp.concatenate([kv_all[t, 0:256, :] for t in group], axis=0)
            return jnp.dot(keys, queries, preferred_element_type=f32)

        s = scores(groups_here[0])
        for i, group in enumerate(groups_here):
            following = scores(groups_here[i + 1]) if i + 1 < len(groups_here) else None
            newest = jnp.maximum(m, jnp.max(s, axis=0, keepdims=True))
            p = jnp.exp(s - newest).astype(bf16)
            factor = jnp.exp(m - newest)
            values = jnp.concatenate(
                [kv_all[t, 256 + 128 * b : 384 + 128 * b, :] for t in group for b in range(2)], axis=1
            )
            values = jnp.concatenate([values, jnp.ones((16, values.shape[1]), bf16)], axis=0)
            product = jnp.dot(values, p, preferred_element_type=f32)
            l = l * factor + product[128:129]
            acc[first] = acc[first] * factor[:, 0:512] + product[0:128, 0:512]
            acc[second] = acc[second] * factor[:, 512:1024] + product[0:128, 512:1024]
            m, s = newest, following
        m_ref[first] = m[:, 0:512]
        m_ref[second] = m[:, 512:1024]
        l_ref[first] = l[:, 0:512]
        l_ref[second] = l[:, 512:1024]

    def unit(n, carry):
        for start, level, i in tasks:

            @pl.when(n == start)
            def _():
                received(level, i)

        third = (n + 1) % 3
        turn = jnp.where(n < 2, n, jnp.where(n < 14, ((n - 2) // 3) % 2, n - 14))
        gz = (turn + me.g[1]) % 2
        single = jnp.where(third == 0, 1, jnp.where(third == 1, 2, 4))
        double = jnp.where(third == 0, 3, jnp.where(third == 1, 5, 6))
        rel = jnp.where(n < 2, 0, jnp.where(n < 8, single, jnp.where(n < 14, double, 7)))
        for half in range(2):
            j = 2 * gz + half
            arrival(kv_all.at[tile_at(j, rel, 1 - me.tp)], sib_recv.at[j, rel])
        a_there = flipped(me.a, rel)
        tiles = [sp_of(a_there, (gz, y, x)) for y in range(2) for x in range(2)]
        far = rel // 4 == 1

        def two_queries(k, inner):
            needed = jnp.where(k == 0, gz == 0, far & ((me.a[0] + gz) % 2 == 1))

            @pl.when(needed)
            def _():
                pair_step(tiles, jnp.where(k == 0, 2, 2 * gz))

            return inner

        lax.fori_loop(0, 2, two_queries, 0)

        def one_query(upper_q, inner):
            j = 2 * gz + upper_q
            upper_q = upper_q == 1
            s_own = tile_at(j, 0, me.tp)
            near = jnp.logical_not(far)
            side = (rel // 2) % 2 == 1
            fits = (me.a[1] + j % 2) % 2 == 1

            @pl.when(near & side & upper_q & fits)
            def _():
                tiles_step(tiles, j)

            @pl.when(near & ((side & (upper_q != fits)) | (jnp.logical_not(side) & upper_q)))
            def _():
                tiles_step(tiles[0:2], j)

            @pl.when(near & jnp.logical_not(side))
            def _():
                def one(i, c):
                    t = sp_of(a_there, (gz, j % 2, i))

                    @pl.when(t < s_own)
                    def _():
                        tiles_step([t], j)

                    return c

                lax.fori_loop(0, 2, one, 0)

            return inner

        return lax.fori_loop(0, 2, one_query, carry)

    lax.fori_loop(0, 16, unit, 0)

    def finish(j, carry):
        inverse = 1.0 / l_ref[j]
        lam = lam_all[0, 0:1, :]
        for b in range(2):
            at_one, at_two = slice(128 * b, 128 * b + 128), slice(256 + 128 * b, 384 + 128 * b)
            out = acc[j, :, at_one] * inverse[:, at_one] - acc[j, :, at_two] * (lam * inverse[:, at_two])
            mean = jnp.mean(out * out, axis=0, keepdims=True)
            out = (out * lax.rsqrt(mean + epsilon)).T * gain_in[...]
            att_send[j, b] = out.astype(bf16)
        chip = tile_at(j, 0, me.tp)
        for b in range(2):
            itself = (chip == me.sp) & (me.tp == b)

            @pl.when(itself)
            def _():
                pltpu.make_async_copy(att_send.at[j, b], att_recv.at[me.head], att_rsem.at[me.head]).start()

            @pl.when(jnp.logical_not(itself))
            def _():
                remote(
                    att_send.at[j, b], att_recv.at[me.head], att_ssem.at[j, b], att_rsem.at[me.head], (chip, b)
                ).start()

        return carry

    lax.fori_loop(0, 4, finish, 0)

    own_copies[3].wait()
    for h in range(8):
        arrival(att_recv.at[h], att_rsem.at[h])
    attended = jnp.concatenate([att_recv[h] for h in range(8)], axis=1)

    def project(n, square):
        at = pl.ds(pl.multiple_of(n * 512, 512), 512)
        value = res_in[:, at].astype(f32) + jnp.dot(attended, ow[:, at], preferred_element_type=f32)
        value = value.astype(bf16)
        after[:, at] = value
        value = value.astype(f32)
        return square + jnp.sum(value * value, axis=1, keepdims=True)

    square = lax.fori_loop(0, 4, project, jnp.zeros((128, 1), f32))
    inverse = lax.rsqrt(square * (1.0 / WIDTH) + epsilon)

    def norm(n, carry):
        at = pl.ds(pl.multiple_of(n * 512, 512), 512)
        routed[:, at] = (after[:, at].astype(f32) * inverse * ng_in[:, at]).astype(bf16)
        return carry

    lax.fori_loop(0, 4, norm, 0)

    def packed(value, into, blk):
        rows = pl.ds(pl.multiple_of(blk * 256, 256), 256)
        for c in range(3):
            stacked = jnp.concatenate(
                [value[c * 32 : c * 32 + 32, k * 256 : k * 256 + 256] for k in range(8)], axis=0
            )
            block = jnp.dot(perm_back[...], stacked, preferred_element_type=f32).astype(bf16)
            into[pl.ds(blk * 16, 16), :, c * 256 : c * 256 + 256] = block.reshape(16, 16, 256)

    def unpacked(source, blk, extra):
        parts = []
        for c in range(3):
            block = source[pl.ds(blk * 16, 16), :, c * 256 : c * 256 + 256].reshape(256, 256)
            parts.append(jnp.dot(perm[...], block, preferred_element_type=f32).astype(bf16))
        columns = []
        for k in range(8):
            pieces = [part[k * 32 : k * 32 + 32, :] for part in parts]
            if extra:
                pieces.append(jnp.zeros((32, 256), bf16))
            columns.append(jnp.concatenate(pieces, axis=0))
        return jnp.concatenate(columns, axis=1)

    def turn_of(step):
        return jnp.where(step == 0, 0, jnp.where(step == 1, 1, jnp.where(step == 2, 3, 2)))

    def block_to(step):
        return (me.z + turn_of(step)) % 4

    def block_from(step):
        return (me.z + 4 - turn_of(step)) % 4

    def spread(blk, source, target, ssem, rsem):
        def one(i, carry):
            to = blk * 16 + (me.sp + 15 - i) % 16

            @pl.when(to == me.sp)
            def _():
                pltpu.make_async_copy(source.at[to], target.at[me.sp], rsem.at[me.sp]).start()

            @pl.when(to != me.sp)
            def _():
                remote(source.at[to], target.at[me.sp], ssem.at[to], rsem.at[me.sp], (to, me.tp)).start()

            return carry

        lax.fori_loop(0, 16, one, 0)

    def collect(blk, target, rsem):
        def one(i, carry):
            arrival(target.at[blk * 16 + i], rsem.at[blk * 16 + i])
            return carry

        lax.fori_loop(0, 16, one, 0)

    def dispatch(step, carry):
        blk = block_to(step)
        rows = pl.ds(pl.multiple_of(blk * 128, 128), 128)
        value = jnp.dot(pick[rows, :], routed[...], preferred_element_type=f32).astype(bf16)
        packed(value, out_buf, blk)
        spread(blk, out_buf, arr_buf, d_send, d_recv)
        return carry

    lax.fori_loop(0, 4, dispatch, 0)

    for c in own_copies[:3]:
        c.wait()
    for c in w_copies:
        c.wait()

    def work(step, carry):
        blk = block_from(step)
        collect(blk, arr_buf, d_recv)
        x = unpacked(arr_buf, blk, False)
        hidden = []
        for half in range(2):
            g = jnp.dot(x, gate[half], preferred_element_type=f32)
            u = jnp.dot(x, up[half], preferred_element_type=f32)
            hidden.append((g * jax.nn.sigmoid(g) * u).astype(bf16))
        y = jnp.dot(hidden[0], down[0], preferred_element_type=f32) + jnp.dot(
            hidden[1], down[1], preferred_element_type=f32
        )
        packed(y.astype(bf16), ret_buf, blk)
        spread(blk, ret_buf, got_buf, r_send, r_recv)
        return carry

    lax.fori_loop(0, 4, work, 0)

    made = []
    for blk in range(4):
        collect(blk, got_buf, r_recv)
        made.append(unpacked(got_buf, blk, True))
    for n in range(4):
        at = slice(n * 512, n * 512 + 512)
        column = jnp.concatenate([part[:, at] for part in made], axis=0)
        both = jnp.dot(blend[...], column, preferred_element_type=f32)
        out_ref[:, at] = (after[:, at].astype(f32) + (both[0:128] + both[128:256])).astype(bf16)

    drain_heads()
    drain_keys()
    drain_rows(out_buf, d_send)
    drain_rows(ret_buf, r_send)


def on_device(
    residual, query_one, key_one, query_two, key_two, value_rows, lambda_head, head_gain, out_weight,
    norm_gain, route_ids, route_weights, gate_weight, up_weight, down_weight,
):
    vmem = pl.BlockSpec(memory_space=pltpu.VMEM)
    smem = pl.BlockSpec(memory_space=pltpu.SMEM)
    anywhere = pl.BlockSpec(memory_space=pl.ANY)
    dma = pltpu.SemaphoreType.DMA
    V = pltpu.VMEM
    return pl.pallas_call(
        layer_kernel,
        out_shape=jax.ShapeDtypeStruct(residual.shape, bf16),
        in_specs=[vmem] * 5 + [smem] + [vmem] * 5 + [anywhere] * 4,
        out_specs=vmem,
        scratch_shapes=[
            V((4, 512, 128), bf16), V((4, 256, 128), bf16), V((4, 8, 128), f32),
            V((64, 512, 128), bf16), V((4, 256, 128), bf16), V((4, 8, 128), f32),
            V((4, 128, 512), bf16), V((4, 128, 512), f32), V((4, 1, 512), f32), V((4, 1, 512), f32),
            V((4, 2, 128, 128), bf16), V((8, 128, 128), bf16),
            V((1024, WIDTH), bf16), V((2, WIDTH, 256), bf16), V((2, WIDTH, 256), bf16),
            V((2, 256, WIDTH), bf16), V((128, WIDTH), bf16), V((128, WIDTH), bf16),
            V((512, 128), bf16), V((256, 512), bf16), V((256, 256), bf16), V((256, 256), bf16),
            V((64, 16, 768), bf16), V((64, 16, 768), bf16), V((64, 16, 768), bf16), V((64, 16, 768), bf16),
            dma((3, 4)), dma((3, 4)), dma((4, 8)), dma((4, 8)), dma((4, 8)), dma((4, 8)),
            dma((4, 2)), dma((8,)), dma((4,)), dma((3,)), dma((3,)),
            dma((64,)), dma((64,)), dma((64,)), dma((64,)),
        ],
        compiler_params=pltpu.CompilerParams(
            collective_id=0, has_side_effects=True, vmem_limit_bytes=56 * 1024 * 1024
        ),
        name="layer",
    )(
        query_one, key_one, query_two, key_two, value_rows, lambda_head, head_gain[None, :], residual,
        norm_gain[None, :], route_ids.T, route_weights.T, out_weight, gate_weight, up_weight, down_weight,
    )


def solution(mesh):
    placed = (
        P(("sp", "tp"), None),
        P("sp", "tp"),
        P("sp", "tp"),
        P("sp", "tp"),
        P("sp", "tp"),
        P("sp", "tp"),
        P("tp"),
        P(),
        P(),
        P(),
        P(("sp", "tp"), None),
        P(("sp", "tp"), None),
        P("sp", None, "tp"),
        P("sp", None, "tp"),
        P("sp", "tp", None),
    )
    return jax.shard_map(
        on_device, mesh=mesh, in_specs=placed, out_specs=P(("sp", "tp"), None), check_vma=False
    )
```

```python
import jax
import jax.numpy as jnp
from jax import lax
from jax.experimental import pallas as pl
from jax.experimental.pallas import tpu as pltpu
from jax.sharding import PartitionSpec as P

epsilon = 1e-06
low_value = -1e30
MESH = pl.DeviceIdType.MESH
CAP = 6
WIDTH = 2048
SINGLES = (1, 2, 4)
f32 = jnp.float32
bf16 = jnp.bfloat16


def to_class(p):
    return ((p + 1) // 2) % 2, p // 2


def to_coord(a, g):
    return 2 * g + (a + g) % 2


def sp_of(a, g):
    return to_coord(a[0], g[0]) * 16 + to_coord(a[1], g[1]) * 4 + to_coord(a[2], g[2])


def flipped(a, mask):
    return ((a[0] + mask // 4) % 2, (a[1] + (mask // 2) % 2) % 2, (a[2] + mask % 2) % 2)


class Place:
    def __init__(self):
        self.sp = lax.axis_index("sp")
        self.tp = lax.axis_index("tp")
        coords = (self.sp // 16, (self.sp // 4) % 4, self.sp % 4)
        pairs = [to_class(p) for p in coords]
        self.z = coords[0]
        self.a = tuple(p[0] for p in pairs)
        self.g = tuple(p[1] for p in pairs)
        self.parity = (self.g[0] + self.g[1] + self.g[2]) % 2
        self.head = self.g[0] * 4 + self.g[1] * 2 + self.g[2]

    def source_g(self, j, core):
        gz, gy = j // 2, j % 2
        return (gz, gy, (core + gz + gy) % 2)


def remote(src, dst, send, recv, device):
    return pltpu.make_async_remote_copy(
        src_ref=src, dst_ref=dst, send_sem=send, recv_sem=recv, device_id=device, device_id_type=MESH
    )


def arrival(at, sem):
    pltpu.make_async_copy(at, at, sem).wait()


def iota(shape, dim):
    return lax.broadcasted_iota(jnp.int32, shape, dim)


def layer_kernel(
    q1_in, k1_in, q2_in, k2_in, v_in, lam_in, gain_in, res_in, ng_in, ids_in, rw_in,
    ow_in, gate_in, up_in, down_in,
    out_ref,
    kv_own, q_own, lam_own, kv_all, q_all, lam_all, q_wide, acc, m_ref, l_ref, att_send, att_recv,
    ow, gate, up, down, after, routed, pick, blend, perm, perm_back, out_buf, arr_buf, ret_buf, got_buf,
    s1_send, s1_recv, s2_send, s2_recv, sib_send, sib_recv, att_ssem, att_rsem,
    w_local, w_send, w_recv, d_send, d_recv, r_send, r_recv,
):
    me = Place()
    sibling = (me.sp, 1 - me.tp)
    barrier = pltpu.get_barrier_semaphore()

    @pl.loop(1, 64)
    def _(i):
        pl.semaphore_signal(barrier, inc=1, device_id=((me.sp + i) % 64, me.tp), device_id_type=MESH)

    for g in range(8):
        chip = sp_of(me.a, (g // 4, (g // 2) % 2, g % 2))
        pl.semaphore_signal(barrier, inc=1, device_id=(chip, 1 - me.tp), device_id_type=MESH)

    own_copies = [
        pltpu.make_async_copy(gate_in.at[0], gate.at[0], w_local.at[0]),
        pltpu.make_async_copy(up_in.at[0], up.at[0], w_local.at[1]),
        pltpu.make_async_copy(down_in.at[0], down.at[0], w_local.at[2]),
        pltpu.make_async_copy(ow_in, ow, w_local.at[3]),
    ]
    for c in own_copies:
        c.start()

    lane = iota((256, 128), 1)
    for pair in range(2):
        at = pl.ds(pair * 128, 128)
        k1, k2 = k1_in[:, at].astype(f32), k2_in[:, at].astype(f32)
        q1, q2 = q1_in[:, at].astype(f32) * 0.125, q2_in[:, at].astype(f32) * 0.125
        for odd in range(2):
            hl = pair * 2 + odd
            if odd:
                keys = jnp.where(lane < 64, pltpu.roll(k1, 64, 1), k2)
                queries = jnp.where(lane < 64, pltpu.roll(q1, 64, 1), q2)
            else:
                keys = jnp.where(lane < 64, k1, pltpu.roll(k2, 64, 1))
                queries = jnp.where(lane < 64, q1, pltpu.roll(q2, 64, 1))
            kv_own[hl, 0:256, :] = keys.astype(bf16)
            for b in range(2):
                rows = slice(b * 128, b * 128 + 128)
                value = v_in[rows, hl * 128 : hl * 128 + 128].astype(f32)
                kv_own[hl, 256 + b * 128 : 384 + b * 128, :] = value.T.astype(bf16)
                q_own[hl, rows, :] = queries[rows, :].T.astype(bf16)
            lam_own[hl] = jnp.full((8, 128), lam_in[hl], f32)
    pl.semaphore_wait(barrier, 71)

    j_me = me.g[0] * 2 + me.g[1]

    def first_target(hl):
        chip = sp_of(me.a, (me.tp, hl // 2, hl % 2))
        return chip, (chip == me.sp) & (me.parity == me.tp)

    def first_sends(kinds):
        for i in range(4):
            hl = ((me.g[0] + i // 2) % 2) * 2 + (me.g[1] + i % 2) % 2
            chip, itself = first_target(hl)
            every = (
                (kv_own.at[hl], kv_all.at[me.sp]),
                (q_own.at[hl], q_all.at[j_me]),
                (lam_own.at[hl], lam_all.at[j_me]),
            )

            @pl.when(itself)
            def _():
                for n in kinds:
                    pltpu.make_async_copy(*every[n], s1_recv.at[n, j_me]).start()

            @pl.when(jnp.logical_not(itself))
            def _():
                for n in kinds:
                    remote(*every[n], s1_send.at[n, hl], s1_recv.at[n, j_me], (chip, me.parity)).start()

    first_sends((0,))
    first_sends((1, 2))

    ids0, ids1 = ids_in[0:1, :], ids_in[1:2, :]
    rw0, rw1 = rw_in[0:1, :], rw_in[1:2, :]
    upper = jnp.where(iota((128, 128), 0) < iota((128, 128), 1), 1.0, 0.0).astype(bf16)
    small = iota((128, 128), 0)
    for blk in range(4):
        expert = blk * 16 + (small % 32) // 2
        place = (small // 32) * 2 + small % 2
        hit0, hit1 = ids0 == expert, ids1 == expert
        hit = jnp.where(hit0 | hit1, 1.0, 0.0)
        rank = jnp.dot(hit.astype(bf16), upper, preferred_element_type=f32)
        chosen = jnp.where(rank == place.astype(f32), hit, 0.0)
        pick[blk * 128 : blk * 128 + 128, :] = chosen.astype(bf16)
        share = chosen * (jnp.where(hit0, rw0, 0.0) + jnp.where(hit1, rw1, 0.0))
        share = share.T
        high = share.astype(bf16)
        blend[0:128, blk * 128 : blk * 128 + 128] = high
        blend[128:256, blk * 128 : blk * 128 + 128] = (share - high.astype(f32)).astype(bf16)
    ia, ib = iota((256, 256), 0), iota((256, 256), 1)
    packed_a = ((ia // 2) % 16) * 16 + (ia % 2) * 8 + ia // 32
    packed_b = ((ib // 2) % 16) * 16 + (ib % 2) * 8 + ib // 32
    perm[...] = jnp.where(packed_a == ib, 1.0, 0.0).astype(bf16)
    perm_back[...] = jnp.where(packed_b == ia, 1.0, 0.0).astype(bf16)

    w_copies = [
        remote(src.at[0], dst.at[1], w_send.at[n], w_recv.at[n], sibling)
        for n, (src, dst) in enumerate(((gate_in, gate), (up_in, up), (down_in, down)))
    ]

    def tile_at(j, rel, core):
        return sp_of(flipped(me.a, rel), me.source_g(j, core))

    def hop(j, rel, bit):
        target = (sp_of(flipped(me.a, bit), me.g), me.tp)
        at = kv_all.at[tile_at(j, rel, me.tp)]
        return remote(at, at, s2_send.at[j, rel + bit], s2_recv.at[j, rel + bit], target)

    def source_at(i):
        return ((me.g[1] + i // 2) % 2) * 2 + (me.g[2] + i % 2) % 2

    def bits_of(j):
        first = jnp.where(j == 3, me.tp, j)
        turns = [(first + p) % 3 for p in range(3)]
        return [(k * k + k + 2) // 2 for k in turns]

    def across(j, rel):
        at = kv_all.at[tile_at(j, rel, me.tp)]
        return remote(at, at, sib_send.at[j, rel], sib_recv.at[j, rel], sibling)

    def drain_first():
        for hl in range(4):
            @pl.when(jnp.logical_not(first_target(hl)[1]))
            def _():
                for n, src in enumerate((kv_own, q_own, lam_own)):
                    arrival(src.at[hl], s1_send.at[n, hl])

    def drain_keys():
        for j in range(4):
            for rel in range(8):
                if rel:
                    arrival(kv_all.at[tile_at(j, 0, me.tp)], s2_send.at[j, rel])
                arrival(kv_all.at[tile_at(j, rel, me.tp)], sib_send.at[j, rel])
        drain_first()

    def drain_heads():
        for j in range(4):
            chip = tile_at(j, 0, me.tp)
            for b in range(2):

                @pl.when(jnp.logical_not((chip == me.sp) & (me.tp == b)))
                def _():
                    arrival(att_send.at[j, b], att_ssem.at[j, b])

    def drain_rows(buffer, sem):
        @pl.loop(0, 64)
        def _(i):
            @pl.when(i != me.sp)
            def _():
                arrival(buffer.at[i], sem.at[i])

    for i in range(4):
        j = source_at(i)
        arrival(kv_all.at[tile_at(j, 0, me.tp)], s1_recv.at[0, j])
        for bit in SINGLES:
            hop(j, 0, bit).start()
        across(j, 0).start()
    for c in w_copies:
        c.start()

    def received(level, i):
        j = source_at(i)
        bits = bits_of(j)
        sets = (((0,), (1,), (2,)), ((0, 1), (0, 2), (1, 2)), ((0, 1, 2),))[level]
        for places in sets:
            rel = sum(bits[p] for p in places)
            arrival(kv_all.at[tile_at(j, rel, me.tp)], s2_recv.at[j, rel])
            for p in range(places[-1] + 1, 3):
                hop(j, rel, bits[p]).start()
            across(j, rel).start()

    for j in range(4):
        arrival(q_all.at[j], s1_recv.at[1, j])
        arrival(lam_all.at[j], s1_recv.at[2, j])


    def diagonal(j, carry):
        full = jnp.concatenate([q_all[j, 0:128, :], q_all[j, 128:256, :]], axis=1)
        row = iota((128, 256), 0)
        zero = jnp.zeros_like(full)
        q_wide[j, :, 0:256] = jnp.where(row < 64, full, zero)
        q_wide[j, :, 256:512] = jnp.where(row >= 64, full, zero)
        t = tile_at(j, 0, me.tp)
        s = jnp.dot(kv_all[t, 0:256, :], q_wide[j], preferred_element_type=f32)
        s = jnp.where(iota(s.shape, 0) <= iota(s.shape, 1) % 256, s, low_value)
        m = jnp.max(s, axis=0, keepdims=True)
        p = jnp.exp(s - m)
        m_ref[j] = m
        l_ref[j] = jnp.sum(p, axis=0, keepdims=True)
        values = jnp.concatenate([kv_all[t, 256:384, :], kv_all[t, 384:512, :]], axis=1)
        acc[j] = jnp.dot(values, p.astype(bf16), preferred_element_type=f32)
        return carry

    received(0, 0)
    lax.fori_loop(0, 4, diagonal, 0, unroll=2)

    def tiles_step(tiles, j):
        m, l = m_ref[j], l_ref[j]
        groups_here = [tiles[i : i + 2] for i in range(0, len(tiles), 2)]

        def scores(group):
            keys = jnp.concatenate([kv_all[t, 0:256, :] for t in group], axis=0)
            return jnp.dot(keys, q_wide[j], preferred_element_type=f32)

        s = scores(groups_here[0])
        for i, group in enumerate(groups_here):
            following = scores(groups_here[i + 1]) if i + 1 < len(groups_here) else None
            newest = jnp.maximum(m, jnp.max(s, axis=0, keepdims=True))
            p = jnp.exp(s - newest).astype(bf16)
            factor = jnp.exp(m - newest)
            values = jnp.concatenate(
                [kv_all[t, 256 + 128 * b : 384 + 128 * b, :] for t in group for b in range(2)], axis=1
            )
            values = jnp.concatenate([values, jnp.ones((16, values.shape[1]), bf16)], axis=0)
            product = jnp.dot(values, p, preferred_element_type=f32)
            l = l * factor + product[128:129]
            acc[j] = acc[j] * factor + product[0:128]
            m, s = newest, following
        m_ref[j] = m
        l_ref[j] = l

    tasks = ((0, 0, 1), (1, 0, 2), (2, 0, 3), (4, 1, 0), (5, 1, 1), (6, 1, 2), (7, 1, 3),
             (9, 2, 0), (10, 2, 1), (11, 2, 2), (12, 2, 3))

    def pair_step(tiles, first):
        second = first + 1
        m = jnp.concatenate([m_ref[first], m_ref[second]], axis=1)
        l = jnp.concatenate([l_ref[first], l_ref[second]], axis=1)
        queries = jnp.concatenate([q_wide[first], q_wide[second]], axis=1)
        groups_here = [tiles[i : i + 2] for i in range(0, len(tiles), 2)]

        def scores(group):
            keys = jnp.concatenate([kv_all[t, 0:256, :] for t in group], axis=0)
            return jnp.dot(keys, queries, preferred_element_type=f32)

        s = scores(groups_here[0])
        for i, group in enumerate(groups_here):
            following = scores(groups_here[i + 1]) if i + 1 < len(groups_here) else None
            newest = jnp.maximum(m, jnp.max(s, axis=0, keepdims=True))
            p = jnp.exp(s - newest).astype(bf16)
            factor = jnp.exp(m - newest)
            values = jnp.concatenate(
                [kv_all[t, 256 + 128 * b : 384 + 128 * b, :] for t in group for b in range(2)], axis=1
            )
            values = jnp.concatenate([values, jnp.ones((16, values.shape[1]), bf16)], axis=0)
            product = jnp.dot(values, p, preferred_element_type=f32)
            l = l * factor + product[128:129]
            acc[first] = acc[first] * factor[:, 0:512] + product[0:128, 0:512]
            acc[second] = acc[second] * factor[:, 512:1024] + product[0:128, 512:1024]
            m, s = newest, following
        m_ref[first] = m[:, 0:512]
        m_ref[second] = m[:, 512:1024]
        l_ref[first] = l[:, 0:512]
        l_ref[second] = l[:, 512:1024]

    def unit(n, carry):
        for start, level, i in tasks:

            @pl.when(n == start)
            def _():
                received(level, i)

        third = (n + 1) % 3
        turn = jnp.where(n < 2, n, jnp.where(n < 14, ((n - 2) // 3) % 2, n - 14))
        gz = (turn + me.g[1]) % 2
        single = jnp.where(third == 0, 1, jnp.where(third == 1, 2, 4))
        double = jnp.where(third == 0, 3, jnp.where(third == 1, 5, 6))
        rel = jnp.where(n < 2, 0, jnp.where(n < 8, single, jnp.where(n < 14, double, 7)))
        for half in range(2):
            j = 2 * gz + half
            arrival(kv_all.at[tile_at(j, rel, 1 - me.tp)], sib_recv.at[j, rel])
        a_there = flipped(me.a, rel)
        tiles = [sp_of(a_there, (gz, y, x)) for y in range(2) for x in range(2)]
        far = rel // 4 == 1

        def two_queries(k, inner):
            needed = jnp.where(k == 0, gz == 0, far & ((me.a[0] + gz) % 2 == 1))

            @pl.when(needed)
            def _():
                pair_step(tiles, jnp.where(k == 0, 2, 2 * gz))

            return inner

        lax.fori_loop(0, 2, two_queries, 0)

        def one_query(upper_q, inner):
            j = 2 * gz + upper_q
            upper_q = upper_q == 1
            s_own = tile_at(j, 0, me.tp)
            near = jnp.logical_not(far)
            side = (rel // 2) % 2 == 1
            fits = (me.a[1] + j % 2) % 2 == 1

            @pl.when(near & side & upper_q & fits)
            def _():
                tiles_step(tiles, j)

            @pl.when(near & ((side & (upper_q != fits)) | (jnp.logical_not(side) & upper_q)))
            def _():
                tiles_step(tiles[0:2], j)

            @pl.when(near & jnp.logical_not(side))
            def _():
                def one(i, c):
                    t = sp_of(a_there, (gz, j % 2, i))

                    @pl.when(t < s_own)
                    def _():
                        tiles_step([t], j)

                    return c

                lax.fori_loop(0, 2, one, 0)

            return inner

        return lax.fori_loop(0, 2, one_query, carry)

    lax.fori_loop(0, 16, unit, 0)

    def finish(j, carry):
        inverse = 1.0 / l_ref[j]
        lam = lam_all[0, 0:1, :]
        for b in range(2):
            at_one, at_two = slice(128 * b, 128 * b + 128), slice(256 + 128 * b, 384 + 128 * b)
            out = acc[j, :, at_one] * inverse[:, at_one] - acc[j, :, at_two] * (lam * inverse[:, at_two])
            mean = jnp.mean(out * out, axis=0, keepdims=True)
            out = (out * lax.rsqrt(mean + epsilon)).T * gain_in[...]
            att_send[j, b] = out.astype(bf16)
        chip = tile_at(j, 0, me.tp)
        for b in range(2):
            itself = (chip == me.sp) & (me.tp == b)

            @pl.when(itself)
            def _():
                pltpu.make_async_copy(att_send.at[j, b], att_recv.at[me.head], att_rsem.at[me.head]).start()

            @pl.when(jnp.logical_not(itself))
            def _():
                remote(
                    att_send.at[j, b], att_recv.at[me.head], att_ssem.at[j, b], att_rsem.at[me.head], (chip, b)
                ).start()

        return carry

    lax.fori_loop(0, 4, finish, 0)

    own_copies[3].wait()
    for h in range(8):
        arrival(att_recv.at[h], att_rsem.at[h])
    attended = jnp.concatenate([att_recv[h] for h in range(8)], axis=1)

    def project(n, square):
        at = pl.ds(pl.multiple_of(n * 512, 512), 512)
        value = res_in[:, at].astype(f32) + jnp.dot(attended, ow[:, at], preferred_element_type=f32)
        value = value.astype(bf16)
        after[:, at] = value
        value = value.astype(f32)
        return square + jnp.sum(value * value, axis=1, keepdims=True)

    square = lax.fori_loop(0, 4, project, jnp.zeros((128, 1), f32), unroll=4)
    inverse = lax.rsqrt(square * (1.0 / WIDTH) + epsilon)

    def norm(n, carry):
        at = pl.ds(pl.multiple_of(n * 512, 512), 512)
        routed[:, at] = (after[:, at].astype(f32) * inverse * ng_in[:, at]).astype(bf16)
        return carry

    lax.fori_loop(0, 4, norm, 0, unroll=4)

    def packed(value, into, blk):
        rows = pl.ds(pl.multiple_of(blk * 256, 256), 256)
        for c in range(3):
            stacked = jnp.concatenate(
                [value[c * 32 : c * 32 + 32, k * 256 : k * 256 + 256] for k in range(8)], axis=0
            )
            block = jnp.dot(perm_back[...], stacked, preferred_element_type=f32).astype(bf16)
            into[pl.ds(blk * 16, 16), :, c * 256 : c * 256 + 256] = block.reshape(16, 16, 256)

    def unpacked(source, blk, extra):
        parts = []
        for c in range(3):
            block = source[pl.ds(blk * 16, 16), :, c * 256 : c * 256 + 256].reshape(256, 256)
            parts.append(jnp.dot(perm[...], block, preferred_element_type=f32).astype(bf16))
        columns = []
        for k in range(8):
            pieces = [part[k * 32 : k * 32 + 32, :] for part in parts]
            if extra:
                pieces.append(jnp.zeros((32, 256), bf16))
            columns.append(jnp.concatenate(pieces, axis=0))
        return jnp.concatenate(columns, axis=1)

    def turn_of(step):
        return jnp.where(step == 0, 0, jnp.where(step == 1, 1, jnp.where(step == 2, 3, 2)))

    def block_to(step):
        return (me.z + turn_of(step)) % 4

    def block_from(step):
        return (me.z + 4 - turn_of(step)) % 4

    def spread(blk, source, target, ssem, rsem):
        def one(i, carry):
            to = blk * 16 + (me.sp + 15 - i) % 16

            @pl.when(to == me.sp)
            def _():
                pltpu.make_async_copy(source.at[to], target.at[me.sp], rsem.at[me.sp]).start()

            @pl.when(to != me.sp)
            def _():
                remote(source.at[to], target.at[me.sp], ssem.at[to], rsem.at[me.sp], (to, me.tp)).start()

            return carry

        lax.fori_loop(0, 16, one, 0)

    def collect(blk, target, rsem):
        def one(i, carry):
            arrival(target.at[blk * 16 + i], rsem.at[blk * 16 + i])
            return carry

        lax.fori_loop(0, 16, one, 0)

    def dispatch(step, carry):
        blk = block_to(step)
        rows = pl.ds(pl.multiple_of(blk * 128, 128), 128)
        value = jnp.dot(pick[rows, :], routed[...], preferred_element_type=f32).astype(bf16)
        packed(value, out_buf, blk)
        spread(blk, out_buf, arr_buf, d_send, d_recv)
        return carry

    lax.fori_loop(0, 4, dispatch, 0)

    for c in own_copies[:3]:
        c.wait()
    for c in w_copies:
        c.wait()

    def work(step, carry):
        blk = block_from(step)
        collect(blk, arr_buf, d_recv)
        x = unpacked(arr_buf, blk, False)
        hidden = []
        for half in range(2):
            g = jnp.dot(x, gate[half], preferred_element_type=f32)
            u = jnp.dot(x, up[half], preferred_element_type=f32)
            hidden.append((g * jax.nn.sigmoid(g) * u).astype(bf16))
        y = jnp.dot(hidden[0], down[0], preferred_element_type=f32) + jnp.dot(
            hidden[1], down[1], preferred_element_type=f32
        )
        packed(y.astype(bf16), ret_buf, blk)
        spread(blk, ret_buf, got_buf, r_send, r_recv)
        return carry

    lax.fori_loop(0, 4, work, 0)

    made = []
    for blk in range(4):
        collect(blk, got_buf, r_recv)
        made.append(unpacked(got_buf, blk, True))
    for n in range(4):
        at = slice(n * 512, n * 512 + 512)
        column = jnp.concatenate([part[:, at] for part in made], axis=0)
        both = jnp.dot(blend[...], column, preferred_element_type=f32)
        out_ref[:, at] = (after[:, at].astype(f32) + (both[0:128] + both[128:256])).astype(bf16)

    drain_heads()
    drain_keys()
    drain_rows(out_buf, d_send)
    drain_rows(ret_buf, r_send)


def on_device(
    residual, query_one, key_one, query_two, key_two, value_rows, lambda_head, head_gain, out_weight,
    norm_gain, route_ids, route_weights, gate_weight, up_weight, down_weight,
):
    vmem = pl.BlockSpec(memory_space=pltpu.VMEM)
    smem = pl.BlockSpec(memory_space=pltpu.SMEM)
    anywhere = pl.BlockSpec(memory_space=pl.ANY)
    dma = pltpu.SemaphoreType.DMA
    V = pltpu.VMEM
    return pl.pallas_call(
        layer_kernel,
        out_shape=jax.ShapeDtypeStruct(residual.shape, bf16),
        in_specs=[vmem] * 5 + [smem] + [vmem] * 5 + [anywhere] * 4,
        out_specs=vmem,
        scratch_shapes=[
            V((4, 512, 128), bf16), V((4, 256, 128), bf16), V((4, 8, 128), f32),
            V((64, 512, 128), bf16), V((4, 256, 128), bf16), V((4, 8, 128), f32),
            V((4, 128, 512), bf16), V((4, 128, 512), f32), V((4, 1, 512), f32), V((4, 1, 512), f32),
            V((4, 2, 128, 128), bf16), V((8, 128, 128), bf16),
            V((1024, WIDTH), bf16), V((2, WIDTH, 256), bf16), V((2, WIDTH, 256), bf16),
            V((2, 256, WIDTH), bf16), V((128, WIDTH), bf16), V((128, WIDTH), bf16),
            V((512, 128), bf16), V((256, 512), bf16), V((256, 256), bf16), V((256, 256), bf16),
            V((64, 16, 768), bf16), V((64, 16, 768), bf16), V((64, 16, 768), bf16), V((64, 16, 768), bf16),
            dma((3, 4)), dma((3, 4)), dma((4, 8)), dma((4, 8)), dma((4, 8)), dma((4, 8)),
            dma((4, 2)), dma((8,)), dma((4,)), dma((3,)), dma((3,)),
            dma((64,)), dma((64,)), dma((64,)), dma((64,)),
        ],
        compiler_params=pltpu.CompilerParams(
            collective_id=0, has_side_effects=True, vmem_limit_bytes=56 * 1024 * 1024
        ),
        name="layer",
    )(
        query_one, key_one, query_two, key_two, value_rows, lambda_head, head_gain[None, :], residual,
        norm_gain[None, :], route_ids.T, route_weights.T, out_weight, gate_weight, up_weight, down_weight,
    )


def solution(mesh):
    placed = (
        P(("sp", "tp"), None),
        P("sp", "tp"),
        P("sp", "tp"),
        P("sp", "tp"),
        P("sp", "tp"),
        P("sp", "tp"),
        P("tp"),
        P(),
        P(),
        P(),
        P(("sp", "tp"), None),
        P(("sp", "tp"), None),
        P("sp", None, "tp"),
        P("sp", None, "tp"),
        P("sp", "tp", None),
    )
    return jax.shard_map(
        on_device, mesh=mesh, in_specs=placed, out_specs=P(("sp", "tp"), None), check_vma=False
    )
```
